128 devices in a mesh: rep: 2 (over z_hi), fs: 32 (over z_lo, y, x), tp: 2 (over core).
Axes of the slice: x: 4, y: 4, z: 4 (z_hi: 2, z_lo: 2; z = z_hi * 2 + z_lo), core: 2. Of those that a mesh axis runs over, the one named last changes fastest.
Arguments:
- layer_in: bfloat16 [65536, 2048], P(('rep', 'fs'), 'tp'), may hold values from -60 to 60
- mix_gain: bfloat16 [2048], P('tp'), may hold values from 0.099609375 to 1.8984375
- pool_weight: float32 [4, 512, 512], P('tp', None, 'fs'), may hold values from -0.25 to 0.25
- pool_scale: float32 [4, 512], P('tp'), may hold values from 0.1 to 1.9
- out_weight: float32 [2048, 2048], P('tp', 'fs'), may hold values from -0.125 to 0.125
- out_scale: float32 [2048], P('tp'), may hold values from 0.1 to 1.9
- channel_gain: bfloat16 [2048], P('tp'), may hold values from 0.099609375 to 1.8984375
- up_weight: float32 [2048, 2816], P('fs', 'tp'), may hold values from -0.125 to 0.125
- up_scale: float32 [2816], P('tp'), may hold values from 0.1 to 1.9
- gate_weight: float32 [2048, 2816], P('fs', 'tp'), may hold values from -0.125 to 0.125
- gate_scale: float32 [2816], P('tp'), may hold values from 0.1 to 1.9
- conv_weight: float32 [3, 2816], P(None, 'tp'), may hold values from -3 to 3
- down_weight: float32 [2816, 2048], P('tp', 'fs'), may hold values from -0.109375 to 0.109375
- down_scale: float32 [2048], P('tp'), may hold values from 0.1 to 1.9
Outputs:
- layer_out: bfloat16 [65536, 2048], P(('rep', 'fs'), 'tp')
The draws below stay inside these ranges and needn't reach their ends.
All inputs are finite; a program needn't handle non-finite values.
Results may differ from the reference program's by a relative error of at most 0.0095.
Values may be sent and summed in bfloat16 or wider, within the bound.
No kernel may reach another device: no remote copies, remote signals or barrier semaphores. Data moves between devices by JAX's collectives and lax.ppermute only.
A program may use at most 128 MiB of HBM per device.

```python
import jax
import jax.numpy as jnp
from jax import lax

D = 2048
FF = 2816
GROUPS = 4
GROUP_DIM = 512
LENGTH = 256
TOKENS = 65536
N_FS = 32
N_TP = 2


def draw_layer_in(key, part):
    first, second, third = jax.random.split(jax.random.fold_in(key, 11), 3)
    rising = jnp.exp(jnp.log(3.0) * jnp.arange(D, dtype=jnp.float32) / D)
    column = rising * jax.random.uniform(second, (D,), jnp.float32, 0.5, 1.5)
    base = jnp.clip(jax.random.normal(first, (TOKENS, D), jnp.float32), -4.0, 4.0)
    row_scale = jnp.exp(jax.random.uniform(third, (TOKENS, 1), jnp.float32, jnp.log(0.3), jnp.log(3.0)))
    return (base * column[None] * row_scale).astype(jnp.bfloat16)


def block_scale(stream_key, extent, shards, low, top_value):
    def one(dim, parts):
        heights = jax.random.uniform(jax.random.fold_in(jax.random.fold_in(stream_key, 6), dim), (parts,), jnp.float32, low / len(shards), top_value / len(shards))
        return jnp.repeat(jnp.exp(heights), extent[dim] // parts).reshape((-1,) + (1,) * (len(extent) - dim - 1))

    level = one(*shards[0])
    for cut in shards[1:]:
        level = level * one(*cut)
    return level


def bell_draw(own_key, shape, spread, reach, cuts=(), kind=jnp.bfloat16):
    factor_of = block_scale(own_key, shape, cuts, -0.22, 0.18) if cuts else 1.0
    values = jax.random.normal(own_key, shape, jnp.float32) * spread * factor_of
    return jnp.minimum(jnp.maximum(values, -reach), reach).astype(kind)


def setup_inputs(seed: int = 0) -> dict:
    arg_keys = jax.random.split(jax.random.key(seed), 15)
    layer_in = draw_layer_in(jax.random.fold_in(arg_keys[14], 71), 0)
    mix_gain = jnp.clip(1.0 + 0.18 * jax.random.normal(arg_keys[1], (D,), jnp.float32), 0.099609375, 1.8984375).astype(jnp.bfloat16)
    pool_weight = bell_draw(arg_keys[2], (GROUPS, GROUP_DIM, GROUP_DIM), GROUP_DIM ** -0.5, 0.25, ((0, 2), (2, 32)), jnp.float32)
    pool_scale = jnp.clip(1.0 + 0.18 * jax.random.normal(arg_keys[3], (GROUPS, GROUP_DIM), jnp.float32), 0.1, 1.9)
    out_weight = bell_draw(arg_keys[4], (D, D), D ** -0.5, 0.125, ((0, 2), (1, 32)), jnp.float32)
    out_scale = jnp.clip(1.0 + 0.18 * jax.random.normal(arg_keys[5], (D,), jnp.float32), 0.1, 1.9)
    channel_gain = jnp.clip(1.0 + 0.18 * jax.random.normal(arg_keys[6], (D,), jnp.float32), 0.099609375, 1.8984375).astype(jnp.bfloat16)
    up_weight = bell_draw(arg_keys[7], (D, FF), D ** -0.5, 0.125, ((0, 32), (1, 2)), jnp.float32)
    up_scale = jnp.clip(1.0 + 0.18 * jax.random.normal(arg_keys[8], (FF,), jnp.float32), 0.1, 1.9)
    gate_weight = bell_draw(arg_keys[9], (D, FF), D ** -0.5, 0.125, ((0, 32), (1, 2)), jnp.float32)
    gate_scale = jnp.clip(1.0 + 0.18 * jax.random.normal(arg_keys[10], (FF,), jnp.float32), 0.1, 1.9)
    conv_weight = bell_draw(arg_keys[11], (3, FF), 0.577, 3.0, ((1, 2),), jnp.float32)
    down_weight = bell_draw(arg_keys[12], (FF, D), FF ** -0.5, 0.109375, ((0, 2), (1, 32)), jnp.float32)
    down_scale = jnp.clip(1.0 + 0.18 * jax.random.normal(arg_keys[13], (D,), jnp.float32), 0.1, 1.9)
    return dict(layer_in=layer_in, mix_gain=mix_gain, pool_weight=pool_weight, pool_scale=pool_scale, out_weight=out_weight, out_scale=out_scale, channel_gain=channel_gain, up_weight=up_weight, up_scale=up_scale, gate_weight=gate_weight, gate_scale=gate_scale, conv_weight=conv_weight, down_weight=down_weight, down_scale=down_scale)


EPS = 1e-06

def settle(values):
    return lax.optimization_barrier(values.astype(jnp.bfloat16)).astype(jnp.float32)

def band_table(length, window):
    rows = lax.broadcasted_iota(jnp.int32, (length, length), 0)
    cols = lax.broadcasted_iota(jnp.int32, (length, length), 1)
    lower = jnp.maximum(rows - window // 2, 0)
    upper = jnp.minimum(rows - window // 2 + window, length)
    inside = (cols >= lower) & (cols < upper)
    count = (upper[:, :1] - lower[:, :1]).astype(jnp.float32)
    return (inside.astype(jnp.bfloat16), count)

def partial_sums(left, right):
    part = left.shape[1] // N_TP
    total = jnp.zeros((left.shape[0], right.shape[1]), jnp.float32)
    for index in range(N_TP):
        piece = jnp.dot(left[:, index * part:(index + 1) * part], right[index * part:(index + 1) * part], preferred_element_type=jnp.float32)
        total = total + settle(piece)
    return total

def block_layer(block_in, mix_gain, pool_bf, pool_scale, out_bf, out_scale, channel_gain, up_bf, up_scale, gate_bf, gate_scale, conv_weight, down_bf, down_scale):
    rows = block_in.shape[0]
    seqs = rows // LENGTH
    x32 = block_in.astype(jnp.float32)
    normed = settle(x32 * lax.rsqrt(lax.optimization_barrier(jnp.mean(x32 * x32, axis=1, keepdims=True)) + EPS) * mix_gain.astype(jnp.float32))
    grouped_in = normed.reshape(seqs, LENGTH, GROUPS, GROUP_DIM)
    outputs = []
    for group in range(GROUPS):
        band, count = band_table(LENGTH, 2 ** (group + 1))
        piece = grouped_in[:, :, group, :]
        total = jnp.einsum('ij,sjc->sic', band.astype(jnp.float32), piece)
        outputs.append(settle(total / count[None] - piece))
    pooled = jnp.stack(outputs, axis=2)
    grouped = jnp.einsum('slgc,gcd->slgd', pooled, pool_bf.astype(jnp.float32)) * pool_scale[None, None]
    grouped = settle(grouped).astype(jnp.bfloat16).reshape(rows, D)
    mixer_sum = partial_sums(grouped, out_bf)
    middle = (x32 + mixer_sum * out_scale[None]).astype(jnp.bfloat16)
    m32 = middle.astype(jnp.float32)
    chan_normed = (m32 * lax.rsqrt(lax.optimization_barrier(jnp.mean(m32 * m32, axis=1, keepdims=True)) + EPS) * channel_gain.astype(jnp.float32)).astype(jnp.bfloat16)
    lifted = settle(jnp.dot(chan_normed, up_bf, preferred_element_type=jnp.float32) * up_scale[None])
    gated = jnp.dot(chan_normed, gate_bf, preferred_element_type=jnp.float32) * gate_scale[None]
    padded = jnp.pad(lifted.reshape(seqs, LENGTH, FF), ((0, 0), (1, 1), (0, 0)))
    conv = conv_weight[0] * padded[:, :-2] + conv_weight[1] * padded[:, 1:-1] + conv_weight[2] * padded[:, 2:]
    hidden = (jax.nn.gelu(conv).reshape(rows, FF) * gated).astype(jnp.bfloat16)
    chan_sum = partial_sums(hidden, down_bf)
    return (m32 + chan_sum * down_scale[None]).astype(jnp.bfloat16)

def reference(layer_in, mix_gain, pool_weight, pool_scale, out_weight, out_scale, channel_gain, up_weight, up_scale, gate_weight, gate_scale, conv_weight, down_weight, down_scale):
    pool_bf = pool_weight.astype(jnp.bfloat16)
    out_bf = out_weight.astype(jnp.bfloat16)
    up_bf = up_weight.astype(jnp.bfloat16)
    gate_bf = gate_weight.astype(jnp.bfloat16)
    down_bf = down_weight.astype(jnp.bfloat16)
    blocks = layer_in.reshape(N_FS, TOKENS // N_FS, D)

    def one_block(block_in):
        return block_layer(block_in, mix_gain, pool_bf, pool_scale, out_bf, out_scale, channel_gain, up_bf, up_scale, gate_bf, gate_scale, conv_weight, down_bf, down_scale)
    return lax.map(one_block, blocks).reshape(TOKENS, D)
```

```python
import jax
import jax.numpy as jnp
from jax import lax
from jax.sharding import Mesh
from jax.sharding import PartitionSpec as P

LENGTH = 256
FS = ("fs_0", "fs_1", "fs_2")
REP_FS = ("rep", "fs_0", "fs_1", "fs_2")
EPS = 1e-06
SWAP = ((0, 1), (1, 0))


def from_partner(array):
    return lax.ppermute(array, "tp", SWAP)


def of_rep(first, second):
    return jnp.where(lax.axis_index("rep") == 0, first, second)


def everywhere(array):
    return lax.all_gather(array, REP_FS, axis=0, tiled=True)


def nt_dot(left, right):
    return lax.dot_general(left, right, (((1,), (1,)), ((), ())), preferred_element_type=jnp.float32)


def band_table(length, window):
    rows = lax.broadcasted_iota(jnp.int32, (length, length), 0)
    cols = lax.broadcasted_iota(jnp.int32, (length, length), 1)
    lower = jnp.maximum(rows - window // 2, 0)
    upper = jnp.minimum(rows - window // 2 + window, length)
    inside = (cols >= lower) & (cols < upper)
    count = (upper[:, :1] - lower[:, :1]).astype(jnp.float32)
    return (inside.astype(jnp.bfloat16), count)


def pool_group(piece, window):
    band, count = band_table(piece.shape[1], window)
    total = jnp.einsum("ij,sjc->sic", band, piece, preferred_element_type=jnp.float32)
    return (total / count[None] - piece.astype(jnp.float32)).astype(jnp.bfloat16)


def summed_over_tp(terms, me):
    half = terms.shape[1] // 2
    theirs = lax.dynamic_slice_in_dim(terms, (1 - me) * half, half, 1)
    mine = lax.dynamic_slice_in_dim(terms, me * half, half, 1)
    return mine.astype(jnp.float32) + from_partner(theirs).astype(jnp.float32)


def per_device(
    layer_in,
    mix_gain,
    pool_weight,
    pool_scale,
    out_weight,
    out_scale,
    channel_gain,
    up_weight,
    up_scale,
    gate_weight,
    gate_scale,
    conv_weight,
    down_weight,
    down_scale,
):
    rows, half = layer_in.shape
    seqs = rows // LENGTH
    me = lax.axis_index("tp")
    width = half * lax.axis_size("tp")
    groups = pool_weight.shape[0]
    group_width = half // groups
    n_fs = width // out_weight.shape[1]
    cols = out_weight.shape[1]
    out_t = out_weight.astype(jnp.bfloat16).T
    pool_t = pool_weight.astype(jnp.bfloat16).transpose(0, 2, 1)
    mixer_part = of_rep(
        jnp.concatenate([out_t[:, :group_width], pool_t[0]], axis=0),
        jnp.concatenate([out_t[:, group_width:], pool_t[1]], axis=0),
    )
    mixer_all = everywhere(mixer_part).reshape(groups, n_fs, -1, group_width)
    ffn_part = of_rep(up_weight, gate_weight).astype(jnp.bfloat16)
    ffn_all = everywhere(ffn_part)
    up_whole, gate_whole = ffn_all[:width], ffn_all[width:]
    down_t = down_weight.astype(jnp.bfloat16).T
    small = cols // 2
    down_part = of_rep(down_t[:small], down_t[small:])
    down_all = everywhere(down_part).reshape(2, n_fs, small, -1)
    down_whole = down_all.transpose(1, 0, 2, 3).reshape(width, -1)

    x32 = layer_in.astype(jnp.float32)
    squares = jnp.sum(x32 * x32, axis=1)
    squares = (squares + from_partner(squares))[:, None]
    normed = (x32 * lax.rsqrt(squares / width + EPS) * mix_gain.astype(jnp.float32)[None]).astype(
        jnp.bfloat16
    )
    terms = jnp.zeros((rows, width), jnp.float32)
    for local in range(groups):
        cut = slice(local * group_width, (local + 1) * group_width)
        window = jnp.left_shift(jnp.int32(1), me * groups + local + 1)
        pooled = pool_group(normed[:, cut].reshape(seqs, LENGTH, group_width), window)
        pool_mat = mixer_all[local, :, cols:].reshape(group_width, group_width)
        grouped = nt_dot(pooled.reshape(rows, group_width), pool_mat)
        grouped = (grouped * pool_scale[local][None]).astype(jnp.bfloat16)
        terms = terms + nt_dot(grouped, mixer_all[local, :, :cols].reshape(width, group_width))
    mixer_sum = summed_over_tp(terms.astype(jnp.bfloat16), me)
    middle = (x32 + mixer_sum * out_scale[None]).astype(jnp.bfloat16)
    m32 = middle.astype(jnp.float32)
    other = from_partner(middle)
    first = me == 0
    whole_middle = jnp.concatenate(
        [jnp.where(first, middle, other), jnp.where(first, other, middle)], axis=1
    )
    gain_other = from_partner(channel_gain)
    whole_gain = jnp.concatenate(
        [jnp.where(first, channel_gain, gain_other), jnp.where(first, gain_other, channel_gain)]
    )
    whole32 = whole_middle.astype(jnp.float32)
    chan_normed = (
        whole32
        * lax.rsqrt(jnp.mean(whole32 * whole32, axis=1, keepdims=True) + EPS)
        * whole_gain.astype(jnp.float32)[None]
    ).astype(jnp.bfloat16)
    lifted_raw = jnp.dot(chan_normed, up_whole, preferred_element_type=jnp.float32)
    gated_raw = jnp.dot(chan_normed, gate_whole, preferred_element_type=jnp.float32)
    hidden_width = up_weight.shape[1]
    lifted = (lifted_raw * up_scale[None]).astype(jnp.bfloat16)
    padded = jnp.pad(
        lifted.reshape(seqs, LENGTH, hidden_width).astype(jnp.float32), ((0, 0), (1, 1), (0, 0))
    )
    conv = (
        conv_weight[0] * padded[:, :-2]
        + conv_weight[1] * padded[:, 1:-1]
        + conv_weight[2] * padded[:, 2:]
    )
    hidden = (
        jax.nn.gelu(conv).reshape(rows, hidden_width) * (gated_raw * gate_scale[None])
    ).astype(jnp.bfloat16)
    chan_terms = nt_dot(hidden, down_whole)
    chan_sum = summed_over_tp(chan_terms.astype(jnp.bfloat16), me)
    return (m32 + chan_sum * down_scale[None]).astype(jnp.bfloat16)


def solution(mesh):
    torus = Mesh(
        mesh.devices.reshape(mesh.shape["rep"], 2, 4, 4, mesh.shape["tp"]),
        ("rep", "fs_0", "fs_1", "fs_2", "tp"),
    )
    in_specs = (
        P(REP_FS, "tp"),
        P("tp"),
        P("tp", None, FS),
        P("tp", None),
        P("tp", FS),
        P("tp"),
        P("tp"),
        P(FS, "tp"),
        P("tp"),
        P(FS, "tp"),
        P("tp"),
        P(None, "tp"),
        P("tp", FS),
        P("tp"),
    )
    out_specs = P(REP_FS, "tp")
    return jax.shard_map(
        per_device, mesh=torus, in_specs=in_specs, out_specs=out_specs, check_vma=False
    )
```

```python
import functools

import jax
import jax.numpy as jnp
from jax import lax
from jax.experimental import pallas as pl
from jax.experimental.pallas import tpu as pltpu
from jax.sharding import Mesh
from jax.sharding import PartitionSpec as P

LENGTH = 256
FS = ("fs_0", "fs_1", "fs_2")
REP_FS = ("rep", "fs_0", "fs_1", "fs_2")
EPS = 1e-06
SWAP = ((0, 1), (1, 0))


def from_partner(array):
    return lax.ppermute(array, "tp", SWAP)


def of_rep(first, second):
    return jnp.where(lax.axis_index("rep") == 0, first, second)


def everywhere(array):
    return lax.all_gather(array, REP_FS, axis=0, tiled=True)


def nt_dot(left, right):
    return lax.dot_general(left, right, (((1,), (1,)), ((), ())), preferred_element_type=jnp.float32)


def band_table(length, window):
    rows = lax.broadcasted_iota(jnp.int32, (length, length), 0)
    cols = lax.broadcasted_iota(jnp.int32, (length, length), 1)
    lower = jnp.maximum(rows - window // 2, 0)
    upper = jnp.minimum(rows - window // 2 + window, length)
    inside = (cols >= lower) & (cols < upper)
    count = (upper[:, :1] - lower[:, :1]).astype(jnp.float32)
    return (inside.astype(jnp.bfloat16), count)


def pool_group(piece, window):
    band, count = band_table(piece.shape[1], window)
    total = jnp.einsum("ij,sjc->sic", band, piece, preferred_element_type=jnp.float32)
    return (total / count[None] - piece.astype(jnp.float32)).astype(jnp.bfloat16)


def summed_over_tp(terms, me):
    half = terms.shape[1] // 2
    theirs = lax.dynamic_slice_in_dim(terms, (1 - me) * half, half, 1)
    mine = lax.dynamic_slice_in_dim(terms, me * half, half, 1)
    return mine.astype(jnp.float32) + from_partner(theirs).astype(jnp.float32)

LINKS = {
    "xa": ("fs_2", 1, 1),
    "xb": ("fs_2", 3, 3),
    "ya": ("fs_1", 1, 4),
    "yb": ("fs_1", 3, 12),
    "za": (("rep", "fs_0"), 1, 16),
    "zb": (("rep", "fs_0"), 3, 16),
}
ORDERS = (
    ("za", "xa", "xb", "ya", "yb"),
    ("zb", "xb", "xa", "yb", "ya"),
    ("za", "ya", "yb", "xa", "xb"),
    ("zb", "yb", "ya", "xb", "xa"),
)


def across(array, link):
    axes, flip, _ = LINKS[link]
    return lax.ppermute(array, axes, [(k, k ^ flip) for k in range(4)])


def doubled(parts):
    held = [part[None] for part in parts]
    for step in range(5):
        got = [across(part, order[step]) for part, order in zip(held, ORDERS)]
        held = [jnp.concatenate(pair, axis=0) for pair in zip(held, got)]
    return held


def flips(order):
    found = [0]
    for link in order:
        found = found + [k ^ LINKS[link][2] for k in found]
    return found


def place_kernel(cols, own_ref, *refs):
    parts, (out_ref, pool_ref) = refs[:-2], refs[-2:]
    lanes = parts[0].shape[2]
    per_group = pool_ref.shape[2] // lanes
    extra = parts[0].shape[1] - cols
    for p, part in enumerate(parts):
        group, place = divmod(p, per_group)
        for j, flip in enumerate(flips(ORDERS[p])):
            owner = own_ref[0] ^ flip
            out_ref[pl.ds(pl.multiple_of(owner * cols, cols), cols), p * lanes : (p + 1) * lanes] = part[j, :cols]
            pool_ref[
                group, pl.ds(pl.multiple_of(owner * extra, extra), extra), place * lanes : (place + 1) * lanes
            ] = part[j, cols:]


def in_vmem():
    return pl.BlockSpec(memory_space=pltpu.VMEM)


def placed(parts, own, cols, groups, group_width, width):
    half = groups * group_width
    return pl.pallas_call(
        functools.partial(place_kernel, cols),
        out_shape=(
            jax.ShapeDtypeStruct((width, half), jnp.bfloat16),
            jax.ShapeDtypeStruct((groups, group_width, group_width), jnp.bfloat16),
        ),
        in_specs=[pl.BlockSpec(memory_space=pltpu.SMEM)] + [in_vmem()] * len(parts),
        out_specs=(in_vmem(), in_vmem()),
        compiler_params=pltpu.CompilerParams(vmem_limit_bytes=40 << 20),
        name="place",
    )(own, *parts)


def hidden_kernel(x_ref, up_ref, gate_ref, us_ref, gs_ref, taps_ref, hidden_ref):
    wide = up_ref.shape[3]
    both = jnp.concatenate([up_ref[0].reshape(-1, wide), gate_ref[0].reshape(-1, wide)], axis=1)
    product = jnp.dot(x_ref[...], both, preferred_element_type=jnp.float32)
    row = lax.broadcasted_iota(jnp.int32, (LENGTH, wide), 0)
    for k in range(x_ref.shape[0] // LENGTH):
        rows = slice(k * LENGTH, (k + 1) * LENGTH)
        lifted = (product[rows, :wide] * us_ref[...]).astype(jnp.bfloat16).astype(jnp.float32)
        before = jnp.where(row == 0, 0.0, pltpu.roll(lifted, 1, 0))
        after = jnp.where(row == LENGTH - 1, 0.0, pltpu.roll(lifted, LENGTH - 1, 0))
        conv = taps_ref[0:1] * before + taps_ref[1:2] * lifted + taps_ref[2:3] * after
        hidden = jax.nn.gelu(conv) * (product[rows, wide:] * gs_ref[...])
        hidden_ref[rows] = hidden.astype(hidden_ref.dtype)


def hidden_of(x, gathered, cols, up_scale, gate_scale, conv_weight):
    rows, width = x.shape
    wide = 128
    n_fs = gathered.shape[1]
    total = gathered.shape[3]
    weight = lambda rep: pl.BlockSpec((1, n_fs, cols, wide), lambda i: (rep, 0, 0, i))
    lane = lambda n: pl.BlockSpec((n, wide), lambda i: (0, i))
    return pl.pallas_call(
        hidden_kernel,
        grid=(total // wide,),
        out_shape=jax.ShapeDtypeStruct((rows, total), jnp.bfloat16),
        in_specs=[pl.BlockSpec((rows, width), lambda i: (0, 0)), weight(0), weight(1), lane(1), lane(1), lane(3)],
        out_specs=pl.BlockSpec((rows, wide), lambda i: (0, i)),
        compiler_params=pltpu.CompilerParams(vmem_limit_bytes=40 << 20),
        cost_estimate=pl.CostEstimate(
            flops=4 * rows * width * total, bytes_accessed=4 * width * total, transcendentals=rows * total
        ),
        name="hidden",
    )(x, gathered, gathered, up_scale[None], gate_scale[None], conv_weight)


def down_kernel(half_ref, hidden_ref, down_ref, terms_ref):
    reps, blocks, small, depth = down_ref.shape
    weight = down_ref[...].transpose(1, 0, 2, 3).reshape(reps * blocks * small, depth)
    terms_ref[...] = nt_dot(hidden_ref[...], weight).astype(terms_ref.dtype)


def down_half(hidden, gathered, which, cols):
    rows, depth = hidden.shape
    n_fs = gathered.shape[1]
    small = cols // 2
    blocks = 4
    steps = n_fs // 2 // blocks
    return pl.pallas_call(
        down_kernel,
        grid_spec=pltpu.PrefetchScalarGridSpec(
            num_scalar_prefetch=1,
            grid=(steps,),
            in_specs=[
                pl.BlockSpec((rows, depth), lambda n, w: (0, 0)),
                pl.BlockSpec((2, blocks, small, depth), lambda n, w: (0, w[0] * steps + n, cols // small, 0)),
            ],
            out_specs=pl.BlockSpec((rows, blocks * cols), lambda n, w: (0, n)),
        ),
        out_shape=jax.ShapeDtypeStruct((rows, n_fs // 2 * cols), jnp.bfloat16),
        compiler_params=pltpu.CompilerParams(vmem_limit_bytes=40 << 20),
        cost_estimate=pl.CostEstimate(
            flops=rows * depth * n_fs * cols, bytes_accessed=depth * n_fs * cols + 4 * rows * depth, transcendentals=0
        ),
        name="down",
    )(which.reshape(1), hidden, gathered)


def per_device(
    layer_in,
    mix_gain,
    pool_weight,
    pool_scale,
    out_weight,
    out_scale,
    channel_gain,
    up_weight,
    up_scale,
    gate_weight,
    gate_scale,
    conv_weight,
    down_weight,
    down_scale,
):
    rows, half = layer_in.shape
    seqs = rows // LENGTH
    me = lax.axis_index("tp")
    width = half * lax.axis_size("tp")
    groups = pool_weight.shape[0]
    group_width = half // groups
    cols = out_weight.shape[1]
    n_fs = width // cols
    small = cols // 2
    hidden_width = up_weight.shape[1]
    down_t = down_weight.astype(jnp.bfloat16).T
    ffn_part = jnp.concatenate(
        [of_rep(up_weight, gate_weight).astype(jnp.bfloat16), of_rep(down_t[:small], down_t[small:])], axis=0
    )
    ffn_all = everywhere(ffn_part).reshape(2, n_fs, cols + small, hidden_width)
    out_t = out_weight.astype(jnp.bfloat16).T
    pool_t = pool_weight.astype(jnp.bfloat16).transpose(2, 0, 1).reshape(-1, half)
    mixer_part = jnp.concatenate([out_t, pool_t], axis=0)
    lanes = half // len(ORDERS)
    parts = doubled([mixer_part[:, k * lanes : (k + 1) * lanes] for k in range(len(ORDERS))])
    own = lax.axis_index(FS).astype(jnp.int32).reshape(1)
    out_whole, pool_whole = placed(parts, own, cols, groups, group_width, width)

    x32 = layer_in.astype(jnp.float32)
    squares = jnp.sum(x32 * x32, axis=1)
    squares = (squares + from_partner(squares))[:, None]
    normed = (x32 * lax.rsqrt(squares / width + EPS) * mix_gain.astype(jnp.float32)[None]).astype(
        jnp.bfloat16
    )
    grouped = []
    for local in range(groups):
        cut = slice(local * group_width, (local + 1) * group_width)
        window = jnp.left_shift(jnp.int32(1), me * groups + local + 1)
        pooled = pool_group(normed[:, cut].reshape(seqs, LENGTH, group_width), window)
        product = nt_dot(pooled.reshape(rows, group_width), pool_whole[local])
        grouped.append((product * pool_scale[local][None]).astype(jnp.bfloat16))
    terms = nt_dot(jnp.concatenate(grouped, axis=1), out_whole)
    mixer_sum = summed_over_tp(terms.astype(jnp.bfloat16), me)
    middle = (x32 + mixer_sum * out_scale[None]).astype(jnp.bfloat16)
    m32 = middle.astype(jnp.float32)
    other = from_partner(middle)
    first = me == 0
    whole_middle = jnp.concatenate(
        [jnp.where(first, middle, other), jnp.where(first, other, middle)], axis=1
    )
    gain_other = from_partner(channel_gain)
    whole_gain = jnp.concatenate(
        [jnp.where(first, channel_gain, gain_other), jnp.where(first, gain_other, channel_gain)]
    )
    whole32 = whole_middle.astype(jnp.float32)
    chan_normed = (
        whole32
        * lax.rsqrt(jnp.mean(whole32 * whole32, axis=1, keepdims=True) + EPS)
        * whole_gain.astype(jnp.float32)[None]
    ).astype(jnp.bfloat16)
    hidden = hidden_of(chan_normed, ffn_all, cols, up_scale, gate_scale, conv_weight)
    theirs = from_partner(down_half(hidden, ffn_all, 1 - me, cols))
    mine = down_half(hidden, ffn_all, me, cols)
    chan_sum = mine.astype(jnp.float32) + theirs.astype(jnp.float32)
    return (m32 + chan_sum * down_scale[None]).astype(jnp.bfloat16)


def solution(mesh):
    torus = Mesh(
        mesh.devices.reshape(mesh.shape["rep"], 2, 4, 4, mesh.shape["tp"]),
        ("rep", "fs_0", "fs_1", "fs_2", "tp"),
    )
    in_specs = (
        P(REP_FS, "tp"),
        P("tp"),
        P("tp", None, FS),
        P("tp", None),
        P("tp", FS),
        P("tp"),
        P("tp"),
        P(FS, "tp"),
        P("tp"),
        P(FS, "tp"),
        P("tp"),
        P(None, "tp"),
        P("tp", FS),
        P("tp"),
    )
    out_specs = P(REP_FS, "tp")
    return jax.shard_map(
        per_device, mesh=torus, in_specs=in_specs, out_specs=out_specs, check_vma=False
    )
```

```python
import functools

import jax
import jax.numpy as jnp
from jax import lax
from jax.experimental import pallas as pl
from jax.experimental.pallas import tpu as pltpu
from jax.sharding import Mesh
from jax.sharding import PartitionSpec as P


LENGTH = 256
FS = ("fs_0", "fs_1", "fs_2")
REP_FS = ("rep", "fs_0", "fs_1", "fs_2")
EPS = 1e-06
SWAP = ((0, 1), (1, 0))


def from_partner(array):
    return lax.ppermute(array, "tp", SWAP)


def nt_dot(left, right):
    return lax.dot_general(left, right, (((1,), (1,)), ((), ())), preferred_element_type=jnp.float32)


LINKS = {
    "xa": ("fs_2", 1, 1),
    "xb": ("fs_2", 3, 3),
    "ya": ("fs_1", 1, 4),
    "yb": ("fs_1", 3, 12),
    "za": (("rep", "fs_0"), 1, 16),
    "zb": (("rep", "fs_0"), 3, 16),
}
PLANS = {
    "ma": ("xa ya xb", ("yb za", "za yb")),
    "mb": ("ya xa yb", ("xb zb", "zb xb")),
    "u": ("za yb ya", ("xa xb", "xb xa")),
    "g": ("zb xb xa", ("ya yb", "yb ya")),
    "da": ("ya xb yb", ("xa za",)),
    "db": ("xa yb xb", ("ya zb",)),
}


def orders_of(*names):
    return tuple(f"{PLANS[name][0]} {end}" for name in names for end in PLANS[name][1])


def across(array, link):
    axes, flip, _ = LINKS[link]
    return lax.ppermute(array, axes, [(k, k ^ flip) for k in range(4)])


def stack_kernel(dim, first_ref, second_ref, *both_refs):
    count = first_ref.shape[0]
    size = both_refs[0].shape[dim]
    for k, both_ref in enumerate(both_refs):
        cut = slice(k * size, (k + 1) * size)
        place = (slice(None), cut) if dim == 1 else (slice(None), slice(None), cut)
        both_ref[:count] = first_ref[place]
        both_ref[count:] = second_ref[place]


def stacked(first, second, dim=1, pieces=1):
    count, *block = first.shape
    block[dim - 1] //= pieces
    return pl.pallas_call(
        functools.partial(stack_kernel, dim),
        out_shape=[pltpu.VMEM((2 * count, *block), first.dtype)] * pieces,
        in_specs=in_vmem(2),
        out_specs=in_vmem(pieces),
        compiler_params=params(4),
        cost_estimate=cost(0, 4 * first.size * 2),
        name="stack",
    )(*near(first, second))


def gathered_over_fs(group, name, dim):
    links, ends = PLANS[name]
    links = links.split()
    held = group[None]
    for step, link in enumerate(links):
        got = across(held, link)
        if step < len(links) - 1:
            (held,) = stacked(held, got)
    pairs = []
    for part, end in zip(stacked(held, got, dim, len(ends)), ends):
        near, far = end.split()
        got = across(part, near)
        (part,) = stacked(part, got)
        pairs += [part, across(part, far)]
    return pairs


def blocks_of(pairs, orders):
    for p, order in enumerate(orders):
        for j, flip in enumerate(flips(order)):
            side, place = divmod(j, pairs[2 * p].shape[0])
            yield p, pairs[2 * p + side], place, flip


def flips(order):
    found = [0]
    for link in order.split():
        found = found + [k ^ LINKS[link][2] for k in found]
    return found


def at(start, size):
    return pl.ds(pl.multiple_of(start * size, size), size)


def in_vmem(count=1):
    return [pl.BlockSpec(memory_space=pltpu.VMEM)] * count


def near(*arrays):
    return [pltpu.with_memory_space_constraint(array, pltpu.VMEM) for array in arrays]


def in_smem():
    return pl.BlockSpec(memory_space=pltpu.SMEM)


def params(mib=16):
    return pltpu.CompilerParams(vmem_limit_bytes=mib << 20)


def cost(flops, moved):
    return pl.CostEstimate(flops=flops, bytes_accessed=moved, transcendentals=0)


def squares_kernel(x_ref, squares_ref):
    for n in range(x_ref.shape[0] // LENGTH):
        seq = slice(n * LENGTH, (n + 1) * LENGTH)
        x = x_ref[seq].astype(jnp.float32)
        squares_ref[seq] = jnp.broadcast_to(jnp.sum(x * x, axis=1, keepdims=True), (LENGTH, 128))


def squares_of(x):
    return pl.pallas_call(
        squares_kernel,
        out_shape=jax.ShapeDtypeStruct((x.shape[0], 128), jnp.float32),
        in_specs=in_vmem(),
        out_specs=in_vmem()[0],
        compiler_params=params(8),
        cost_estimate=cost(0, 2 * x.size),
        name="squares",
    )(x)


def pool_kernel(spot_ref, x_ref, own_ref, other_ref, gain_ref, pooled_ref):
    rows, half = x_ref.shape
    groups = 2
    span = half // groups
    place = lax.broadcasted_iota(jnp.int32, (LENGTH, LENGTH), 0)
    other = lax.broadcasted_iota(jnp.int32, (LENGTH, LENGTH), 1)
    for k in range(groups):
        reach = jnp.left_shift(jnp.int32(1), spot_ref[1] * groups + k)
        lower = jnp.maximum(place - reach, 0)
        upper = jnp.minimum(place + reach, LENGTH)
        band = jnp.where((other >= lower) & (other < upper), 1.0, 0.0).astype(jnp.bfloat16)
        count = (upper - lower)[:, :1].astype(jnp.float32)
        lane = slice(k * span, (k + 1) * span)
        for n in range(rows // LENGTH):
            seq = slice(n * LENGTH, (n + 1) * LENGTH)
            squares = own_ref[seq, :1] + other_ref[seq, :1]
            scale = lax.rsqrt(squares / (2 * half) + EPS)
            normed = x_ref[seq, lane].astype(jnp.float32) * scale * gain_ref[:, lane].astype(jnp.float32)
            normed = normed.astype(jnp.bfloat16)
            total = jnp.dot(band, normed, preferred_element_type=jnp.float32)
            pooled_ref[seq, lane] = (total / count - normed.astype(jnp.float32)).astype(jnp.bfloat16)


def pooled_of(spot, x, own, other, gain):
    return pl.pallas_call(
        pool_kernel,
        out_shape=jax.ShapeDtypeStruct(x.shape, jnp.bfloat16),
        in_specs=[in_smem(), *in_vmem(4)],
        out_specs=in_vmem()[0],
        compiler_params=params(8),
        cost_estimate=cost(2 * LENGTH * x.size, 4 * x.size),
        name="pool",
    )(spot, x, own, other, gain[None])


def middle_kernel(x_ref, mine_ref, theirs_ref, scale_ref, middle_ref):
    total = mine_ref[...].astype(jnp.float32) + theirs_ref[...].astype(jnp.float32)
    middle_ref[...] = (x_ref[...].astype(jnp.float32) + total * scale_ref[...]).astype(jnp.bfloat16)


def middle_of(x, mine, theirs, scale):
    return pl.pallas_call(
        middle_kernel,
        out_shape=jax.ShapeDtypeStruct(x.shape, jnp.bfloat16),
        in_specs=in_vmem(4),
        out_specs=in_vmem()[0],
        compiler_params=params(8),
        cost_estimate=cost(0, 8 * x.size),
        name="middle",
    )(x, mine, theirs, scale[None])


def norm_kernel(spot_ref, own_ref, other_ref, own_gain_ref, other_gain_ref, normed_ref):
    rows, half = own_ref.shape
    for n in range(rows // LENGTH):
        seq = slice(n * LENGTH, (n + 1) * LENGTH)
        sides = [ref[seq].astype(jnp.float32) for ref in (own_ref, other_ref)]
        squares = sum(jnp.sum(side * side, axis=1, keepdims=True) for side in sides)
        scale = lax.rsqrt(squares / (2 * half) + EPS)
        for core, side, gain in zip((spot_ref[1], 1 - spot_ref[1]), sides, (own_gain_ref, other_gain_ref)):
            normed_ref[seq, at(core, half)] = (side * scale * gain[...].astype(jnp.float32)).astype(jnp.bfloat16)


def normed_of(spot, own, other, own_gain, other_gain):
    rows, half = own.shape
    return pl.pallas_call(
        norm_kernel,
        out_shape=jax.ShapeDtypeStruct((rows, 2 * half), jnp.bfloat16),
        in_specs=[in_smem(), *in_vmem(4)],
        out_specs=in_vmem()[0],
        compiler_params=params(8),
        cost_estimate=cost(0, 8 * own.size),
        name="norm",
    )(spot, own, other, own_gain, other_gain)


def theirs_kernel(cols, spot_ref, pooled_ref, scale_ref, *refs):
    parts, (theirs_ref, grouped_ref, out_ref, pool_ref) = refs[:-4], refs[-4:]
    groups, group_width = pool_ref.shape[:2]
    half = groups * group_width
    lanes = parts[0].shape[2]
    extra = parts[0].shape[1] - cols
    for p, part, j, flip in blocks_of(parts, orders_of("ma", "mb")):
        group, place = divmod(p * lanes, group_width)
        owner = spot_ref[0] ^ flip
        out_ref[at(owner, cols), p * lanes : (p + 1) * lanes] = part[j, :cols]
        pool_ref[group, at(owner, extra), place : place + lanes] = part[j, cols:]
    for k in range(groups):
        span = slice(k * group_width, (k + 1) * group_width)
        product = nt_dot(pooled_ref[:, span], pool_ref[k])
        grouped_ref[:, span] = (product * scale_ref[k : k + 1]).astype(jnp.bfloat16)
    theirs_ref[...] = nt_dot(grouped_ref[...], out_ref[at(1 - spot_ref[1], half), :]).astype(jnp.bfloat16)


def mixer_theirs(spot, pooled, pool_scale, parts, cols, width):
    rows, half = pooled.shape
    groups, group_width = pool_scale.shape
    like = lambda *shape: jax.ShapeDtypeStruct(shape, jnp.bfloat16)
    return pl.pallas_call(
        functools.partial(theirs_kernel, cols),
        out_shape=(like(rows, half), like(rows, half), like(width, half)),
        in_specs=[in_smem(), *in_vmem(2 + len(parts))],
        out_specs=in_vmem(3),
        scratch_shapes=[pltpu.VMEM((groups, group_width, group_width), jnp.bfloat16)],
        compiler_params=params(),
        cost_estimate=cost(2 * rows * half * (half + group_width), 4 * rows * half),
        name="mixer_theirs",
    )(spot, pooled, pool_scale, *near(*parts))


def mine_kernel(spot_ref, left_ref, right_ref, mine_ref):
    half = mine_ref.shape[1]
    mine_ref[...] = nt_dot(left_ref[...], right_ref[at(spot_ref[1], half), :]).astype(jnp.bfloat16)


def mine_of(spot, left, right):
    rows, depth = left.shape
    half = right.shape[0] // 2
    return pl.pallas_call(
        mine_kernel,
        out_shape=jax.ShapeDtypeStruct((rows, half), jnp.bfloat16),
        in_specs=[in_smem(), *in_vmem(2)],
        out_specs=in_vmem()[0],
        compiler_params=params(),
        cost_estimate=cost(2 * rows * depth * half, 4 * rows * half),
    )(spot, left, right)


def hidden_kernel(spot_ref, x_ref, us_ref, gs_ref, taps_ref, *refs):
    parts, (hidden_ref, weight_ref) = refs[:-2], refs[-2:]
    size = parts[0].shape[1]
    wide = weight_ref.shape[1] // 2
    row = lax.broadcasted_iota(jnp.int32, (LENGTH, wide), 0)

    def tile(i, carry):
        lane = at(i, wide)
        for p, part, j, flip in blocks_of(parts, orders_of("u", "g")):
            side, piece = divmod(p, 2)
            block = (spot_ref[0] ^ flip) * 2 + piece
            weight_ref[at(block, size), side * wide : (side + 1) * wide] = part[j, :, lane]
        product = jnp.dot(x_ref[...], weight_ref[...], preferred_element_type=jnp.float32)
        for k in range(x_ref.shape[0] // LENGTH):
            rows = slice(k * LENGTH, (k + 1) * LENGTH)
            lifted = (product[rows, :wide] * us_ref[:, lane]).astype(jnp.bfloat16).astype(jnp.float32)
            before = jnp.where(row == 0, 0.0, pltpu.roll(lifted, 1, 0))
            after = jnp.where(row == LENGTH - 1, 0.0, pltpu.roll(lifted, LENGTH - 1, 0))
            conv = taps_ref[0:1, lane] * before + taps_ref[1:2, lane] * lifted + taps_ref[2:3, lane] * after
            hidden = jax.nn.gelu(conv) * (product[rows, wide:] * gs_ref[:, lane])
            hidden_ref[rows, lane] = hidden.astype(hidden_ref.dtype)
        return carry

    lax.fori_loop(0, hidden_ref.shape[1] // wide, tile, 0)


def hidden_of(spot, x, up_scale, gate_scale, conv_weight, parts):
    rows, width = x.shape
    total = parts[0].shape[2]
    return pl.pallas_call(
        hidden_kernel,
        out_shape=jax.ShapeDtypeStruct((rows, total), jnp.bfloat16),
        in_specs=[in_smem(), *in_vmem(4 + len(parts))],
        out_specs=in_vmem()[0],
        scratch_shapes=[pltpu.VMEM((width, 256), jnp.bfloat16)],
        compiler_params=params(),
        cost_estimate=cost(4 * rows * width * total, 4 * rows * width),
        name="hidden",
    )(spot, x, up_scale[None], gate_scale[None], conv_weight, *near(*parts))


def down_kernel(spot_ref, hidden_ref, *refs):
    parts, (theirs_ref, mine_ref, weight_ref) = refs[:-3], refs[-3:]
    size = parts[0].shape[1]
    near = spot_ref[0] ^ (spot_ref[1] * 16)
    for p, part, j, flip in blocks_of(parts, orders_of("da", "db")):
        owner = near ^ flip
        block = (owner & 15) * 2 + p

        @pl.when(owner >= 16)
        def _(part=part, j=j, block=block):
            weight_ref[at(block, size), :] = part[j]

        @pl.when(owner < 16)
        def _(part=part, j=j, block=block):
            mine_ref[at(block, size), :] = part[j]

    theirs_ref[...] = nt_dot(hidden_ref[...], weight_ref[...]).astype(theirs_ref.dtype)


def down_theirs(spot, hidden, parts, width):
    rows, depth = hidden.shape
    half = width // 2
    like = lambda *shape: jax.ShapeDtypeStruct(shape, jnp.bfloat16)
    return pl.pallas_call(
        down_kernel,
        out_shape=(like(rows, half), like(half, depth)),
        in_specs=[in_smem(), *in_vmem(1 + len(parts))],
        out_specs=in_vmem(2),
        scratch_shapes=[pltpu.VMEM((half, depth), jnp.bfloat16)],
        compiler_params=params(),
        cost_estimate=cost(rows * depth * width, 4 * rows * depth),
        name="down_theirs",
    )(spot, hidden, *near(*parts))


def terms_kernel(left_ref, right_ref, terms_ref):
    terms_ref[...] = nt_dot(left_ref[...], right_ref[...]).astype(terms_ref.dtype)


def terms_of(left, right):
    rows, depth = left.shape
    half = right.shape[0]
    return pl.pallas_call(
        terms_kernel,
        out_shape=jax.ShapeDtypeStruct((rows, half), jnp.bfloat16),
        in_specs=in_vmem(2),
        out_specs=in_vmem()[0],
        compiler_params=params(),
        cost_estimate=cost(2 * rows * depth * half, 4 * rows * half),
        name="down_mine",
    )(left, right)


def final_kernel(middle_ref, mine_ref, theirs_ref, scale_ref, out_ref):
    rows = at(pl.program_id(0), out_ref.shape[0])
    total = mine_ref[rows].astype(jnp.float32) + theirs_ref[rows].astype(jnp.float32)
    out_ref[...] = (middle_ref[rows].astype(jnp.float32) + total * scale_ref[...]).astype(out_ref.dtype)


def final_of(middle, mine, theirs, scale):
    rows, half = middle.shape
    return pl.pallas_call(
        final_kernel,
        grid=(4,),
        out_shape=jax.ShapeDtypeStruct((rows, half), jnp.bfloat16),
        in_specs=in_vmem(4),
        out_specs=pl.BlockSpec((rows // 4, half), lambda i: (i, 0)),
        compiler_params=params(8),
        cost_estimate=cost(0, 8 * rows * half),
        name="final",
    )(middle, mine, theirs, scale[None])


def per_device(
    layer_in,
    mix_gain,
    pool_weight,
    pool_scale,
    out_weight,
    out_scale,
    channel_gain,
    up_weight,
    up_scale,
    gate_weight,
    gate_scale,
    conv_weight,
    down_weight,
    down_scale,
):
    _, half = layer_in.shape
    me = lax.axis_index("tp")
    width = half * lax.axis_size("tp")
    cols = out_weight.shape[1]
    spot = jnp.stack([lax.axis_index(FS), me]).astype(jnp.int32)
    out_t = out_weight.astype(jnp.bfloat16).T
    pool_t = pool_weight.astype(jnp.bfloat16).transpose(2, 0, 1).reshape(-1, half)
    mixer_part = jnp.concatenate([out_t, pool_t], axis=0)
    lanes = half // 2
    mixer = gathered_over_fs(mixer_part[:, :lanes], "ma", 2) + gathered_over_fs(mixer_part[:, lanes:], "mb", 2)
    wide = gathered_over_fs(up_weight.astype(jnp.bfloat16), "u", 1)
    wide += gathered_over_fs(gate_weight.astype(jnp.bfloat16), "g", 1)
    down_t = down_weight.astype(jnp.bfloat16).T
    down = gathered_over_fs(down_t[: cols // 2], "da", 1) + gathered_over_fs(down_t[cols // 2 :], "db", 1)

    squares = squares_of(layer_in)
    own_gain = channel_gain[None]
    other_gain = from_partner(own_gain)
    pooled = pooled_of(spot, layer_in, squares, from_partner(squares), mix_gain)
    theirs, grouped, out_whole = mixer_theirs(spot, pooled, pool_scale, mixer, cols, width)
    theirs = from_partner(theirs)
    mine = mine_of(spot, grouped, out_whole)
    middle = middle_of(layer_in, mine, theirs, out_scale)
    chan_normed = normed_of(spot, middle, from_partner(middle), own_gain, other_gain)
    hidden = hidden_of(spot, chan_normed, up_scale, gate_scale, conv_weight, wide)
    theirs, down_mine = down_theirs(spot, hidden, down, width)
    theirs = from_partner(theirs)
    return final_of(middle, terms_of(hidden, down_mine), theirs, down_scale)


def solution(mesh):
    torus = Mesh(
        mesh.devices.reshape(mesh.shape["rep"], 2, 4, 4, mesh.shape["tp"]),
        ("rep", "fs_0", "fs_1", "fs_2", "tp"),
    )
    in_specs = (
        P(REP_FS, "tp"),
        P("tp"),
        P("tp", None, FS),
        P("tp", None),
        P("tp", FS),
        P("tp"),
        P("tp"),
        P(FS, "tp"),
        P("tp"),
        P(FS, "tp"),
        P("tp"),
        P(None, "tp"),
        P("tp", FS),
        P("tp"),
    )
    out_specs = P(REP_FS, "tp")
    return jax.shard_map(per_device, mesh=torus, in_specs=in_specs, out_specs=out_specs, check_vma=False)
```

```python
import functools

import jax
import jax.numpy as jnp
from jax import lax
from jax.experimental import pallas as pl
from jax.experimental.pallas import tpu as pltpu
from jax.sharding import Mesh
from jax.sharding import PartitionSpec as P


LENGTH = 256
FS = ("fs_0", "fs_1", "fs_2")
REP_FS = ("rep", "fs_0", "fs_1", "fs_2")
EPS = 1e-06
SWAP = ((0, 1), (1, 0))


def from_partner(array):
    return lax.ppermute(array, "tp", SWAP)


def nt_dot(left, right):
    return lax.dot_general(left, right, (((1,), (1,)), ((), ())), preferred_element_type=jnp.float32)


LINKS = {
    "xa": ("fs_2", 1, 1),
    "xb": ("fs_2", 3, 3),
    "ya": ("fs_1", 1, 4),
    "yb": ("fs_1", 3, 12),
    "za": (("rep", "fs_0"), 1, 16),
    "zb": (("rep", "fs_0"), 3, 16),
}
PLANS = {
    "ma": ("xa xb yb", ("za ya", "ya za",)),
    "mb": ("xa ya yb", ("zb xb", "xb zb",)),
    "u": ("xa xb yb", ("za ya", "ya za",)),
    "g": ("ya zb xb", ("yb xa", "xa yb",)),
    "d": ("yb ya xa", ("xb zb", "zb xb",)),
}


def orders_of(*names):
    return tuple(f"{PLANS[name][0]} {end}" for name in names for end in PLANS[name][1])


def across(array, link):
    axes, flip, _ = LINKS[link]
    return lax.ppermute(array, axes, [(k, k ^ flip) for k in range(4)])


def stack_kernel(dim, first_ref, second_ref, *both_refs):
    count = first_ref.shape[0]
    size = both_refs[0].shape[dim]
    for k, both_ref in enumerate(both_refs):
        cut = slice(k * size, (k + 1) * size)
        place = (slice(None), cut) if dim == 1 else (slice(None), slice(None), cut)
        both_ref[:count] = first_ref[place]
        both_ref[count:] = second_ref[place]


def stacked(first, second, dim=1, pieces=1):
    count, *block = first.shape
    block[dim - 1] //= pieces
    return pl.pallas_call(
        functools.partial(stack_kernel, dim),
        out_shape=[pltpu.VMEM((2 * count, *block), first.dtype)] * pieces,
        in_specs=in_vmem(2),
        out_specs=in_vmem(pieces),
        compiler_params=params(4),
        cost_estimate=cost(0, 4 * first.size * 2),
        name="stack",
    )(*near(first, second))


def gathered_over_fs(group, name, dim):
    links, ends = PLANS[name]
    links = links.split()
    held = group[None]
    for step, link in enumerate(links):
        got = across(held, link)
        if step < len(links) - 1:
            (held,) = stacked(held, got)
    pairs = []
    for part, end in zip(stacked(held, got, dim, len(ends)), ends):
        near, far = end.split()
        got = across(part, near)
        (part,) = stacked(part, got)
        pairs += [part, across(part, far)]
    return pairs


def blocks_of(pairs, orders):
    for p, order in enumerate(orders):
        for j, flip in enumerate(flips(order)):
            side, place = divmod(j, pairs[2 * p].shape[0])
            yield p, pairs[2 * p + side], place, flip


def flips(order):
    found = [0]
    for link in order.split():
        found = found + [k ^ LINKS[link][2] for k in found]
    return found


def at(start, size):
    return pl.ds(pl.multiple_of(start * size, size), size)


def in_vmem(count=1):
    return [pl.BlockSpec(memory_space=pltpu.VMEM)] * count


def near(*arrays):
    return [pltpu.with_memory_space_constraint(array, pltpu.VMEM) for array in arrays]


def in_smem():
    return pl.BlockSpec(memory_space=pltpu.SMEM)


def params(mib=16):
    return pltpu.CompilerParams(vmem_limit_bytes=mib << 20)


def cost(flops, moved):
    return pl.CostEstimate(flops=flops, bytes_accessed=moved, transcendentals=0)


def squares_kernel(x_ref, squares_ref):
    for n in range(x_ref.shape[0] // LENGTH):
        seq = slice(n * LENGTH, (n + 1) * LENGTH)
        x = x_ref[seq].astype(jnp.float32)
        squares_ref[seq] = jnp.broadcast_to(jnp.sum(x * x, axis=1, keepdims=True), (LENGTH, 128))


def squares_of(x):
    return pl.pallas_call(
        squares_kernel,
        out_shape=jax.ShapeDtypeStruct((x.shape[0], 128), jnp.float32),
        in_specs=in_vmem(),
        out_specs=in_vmem()[0],
        compiler_params=params(8),
        cost_estimate=cost(0, 2 * x.size),
        name="squares",
    )(x)


def pool_kernel(spot_ref, x_ref, own_ref, other_ref, gain_ref, pooled_ref):
    rows, half = x_ref.shape
    groups = 2
    span = half // groups
    place = lax.broadcasted_iota(jnp.int32, (LENGTH, LENGTH), 0)
    other = lax.broadcasted_iota(jnp.int32, (LENGTH, LENGTH), 1)
    for k in range(groups):
        reach = jnp.left_shift(jnp.int32(1), spot_ref[1] * groups + k)
        lower = jnp.maximum(place - reach, 0)
        upper = jnp.minimum(place + reach, LENGTH)
        band = jnp.where((other >= lower) & (other < upper), 1.0, 0.0).astype(jnp.bfloat16)
        count = (upper - lower)[:, :1].astype(jnp.float32)
        lane = slice(k * span, (k + 1) * span)
        for n in range(rows // LENGTH):
            seq = slice(n * LENGTH, (n + 1) * LENGTH)
            squares = own_ref[seq, :1] + other_ref[seq, :1]
            scale = lax.rsqrt(squares / (2 * half) + EPS)
            normed = x_ref[seq, lane].astype(jnp.float32) * scale * gain_ref[:, lane].astype(jnp.float32)
            normed = normed.astype(jnp.bfloat16)
            total = jnp.dot(band, normed, preferred_element_type=jnp.float32)
            pooled_ref[seq, lane] = (total / count - normed.astype(jnp.float32)).astype(jnp.bfloat16)


def pooled_of(spot, x, own, other, gain):
    return pl.pallas_call(
        pool_kernel,
        out_shape=jax.ShapeDtypeStruct(x.shape, jnp.bfloat16),
        in_specs=[in_smem(), *in_vmem(4)],
        out_specs=in_vmem()[0],
        compiler_params=params(8),
        cost_estimate=cost(2 * LENGTH * x.size, 4 * x.size),
        name="pool",
    )(spot, x, own, other, gain[None])


def middle_kernel(x_ref, mine_ref, theirs_ref, scale_ref, middle_ref):
    total = mine_ref[...].astype(jnp.float32) + theirs_ref[...].astype(jnp.float32)
    middle_ref[...] = (x_ref[...].astype(jnp.float32) + total * scale_ref[...]).astype(jnp.bfloat16)


def middle_of(x, mine, theirs, scale):
    return pl.pallas_call(
        middle_kernel,
        out_shape=jax.ShapeDtypeStruct(x.shape, jnp.bfloat16),
        in_specs=in_vmem(4),
        out_specs=in_vmem()[0],
        compiler_params=params(8),
        cost_estimate=cost(0, 8 * x.size),
        name="middle",
    )(x, mine, theirs, scale[None])


def norm_kernel(spot_ref, own_ref, other_ref, own_gain_ref, other_gain_ref, normed_ref):
    rows, half = own_ref.shape
    for n in range(rows // LENGTH):
        seq = slice(n * LENGTH, (n + 1) * LENGTH)
        sides = [ref[seq].astype(jnp.float32) for ref in (own_ref, other_ref)]
        squares = sum(jnp.sum(side * side, axis=1, keepdims=True) for side in sides)
        scale = lax.rsqrt(squares / (2 * half) + EPS)
        for core, side, gain in zip((spot_ref[1], 1 - spot_ref[1]), sides, (own_gain_ref, other_gain_ref)):
            normed_ref[seq, at(core, half)] = (side * scale * gain[...].astype(jnp.float32)).astype(jnp.bfloat16)


def normed_of(spot, own, other, own_gain, other_gain):
    rows, half = own.shape
    return pl.pallas_call(
        norm_kernel,
        out_shape=jax.ShapeDtypeStruct((rows, 2 * half), jnp.bfloat16),
        in_specs=[in_smem(), *in_vmem(4)],
        out_specs=in_vmem()[0],
        compiler_params=params(8),
        cost_estimate=cost(0, 8 * own.size),
        name="norm",
    )(spot, own, other, own_gain, other_gain)


def theirs_kernel(cols, spot_ref, pooled_ref, scale_ref, *refs):
    parts, (theirs_ref, grouped_ref, out_ref, pool_ref) = refs[:-4], refs[-4:]
    groups, group_width = pool_ref.shape[:2]
    half = groups * group_width
    lanes = parts[0].shape[2]
    extra = parts[0].shape[1] - cols
    for p, part, j, flip in blocks_of(parts, orders_of("ma", "mb")):
        group, place = divmod(p * lanes, group_width)
        owner = spot_ref[0] ^ flip
        out_ref[at(owner, cols), p * lanes : (p + 1) * lanes] = part[j, :cols]
        pool_ref[group, at(owner, extra), place : place + lanes] = part[j, cols:]
    for k in range(groups):
        span = slice(k * group_width, (k + 1) * group_width)
        product = nt_dot(pooled_ref[:, span], pool_ref[k])
        grouped_ref[:, span] = (product * scale_ref[k : k + 1]).astype(jnp.bfloat16)
    theirs_ref[...] = nt_dot(grouped_ref[...], out_ref[at(1 - spot_ref[1], half), :]).astype(jnp.bfloat16)


def mixer_theirs(spot, pooled, pool_scale, parts, cols, width):
    rows, half = pooled.shape
    groups, group_width = pool_scale.shape
    like = lambda *shape: jax.ShapeDtypeStruct(shape, jnp.bfloat16)
    return pl.pallas_call(
        functools.partial(theirs_kernel, cols),
        out_shape=(like(rows, half), like(rows, half), like(width, half)),
        in_specs=[in_smem(), *in_vmem(2 + len(parts))],
        out_specs=in_vmem(3),
        scratch_shapes=[pltpu.VMEM((groups, group_width, group_width), jnp.bfloat16)],
        compiler_params=params(),
        cost_estimate=cost(2 * rows * half * (half + group_width), 4 * rows * half),
        name="mixer_theirs",
    )(spot, pooled, pool_scale, *near(*parts))


def mine_kernel(spot_ref, left_ref, right_ref, mine_ref):
    half = mine_ref.shape[1]
    mine_ref[...] = nt_dot(left_ref[...], right_ref[at(spot_ref[1], half), :]).astype(jnp.bfloat16)


def mine_of(spot, left, right):
    rows, depth = left.shape
    half = right.shape[0] // 2
    return pl.pallas_call(
        mine_kernel,
        out_shape=jax.ShapeDtypeStruct((rows, half), jnp.bfloat16),
        in_specs=[in_smem(), *in_vmem(2)],
        out_specs=in_vmem()[0],
        compiler_params=params(),
        cost_estimate=cost(2 * rows * depth * half, 4 * rows * half),
    )(spot, left, right)


def hidden_kernel(spot_ref, x_ref, us_ref, gs_ref, taps_ref, *refs):
    parts, (hidden_ref, weight_ref) = refs[:-2], refs[-2:]
    size = parts[0].shape[1]
    wide = weight_ref.shape[1] // 2
    row = lax.broadcasted_iota(jnp.int32, (LENGTH, wide), 0)

    def tile(i, carry):
        lane = at(i, wide)
        for p, part, j, flip in blocks_of(parts, orders_of("u", "g")):
            side, piece = divmod(p, 2)
            block = (spot_ref[0] ^ flip) * 2 + piece
            weight_ref[at(block, size), side * wide : (side + 1) * wide] = part[j, :, lane]
        product = jnp.dot(x_ref[...], weight_ref[...], preferred_element_type=jnp.float32)
        for k in range(x_ref.shape[0] // LENGTH):
            rows = slice(k * LENGTH, (k + 1) * LENGTH)
            lifted = (product[rows, :wide] * us_ref[:, lane]).astype(jnp.bfloat16).astype(jnp.float32)
            before = jnp.where(row == 0, 0.0, pltpu.roll(lifted, 1, 0))
            after = jnp.where(row == LENGTH - 1, 0.0, pltpu.roll(lifted, LENGTH - 1, 0))
            conv = taps_ref[0:1, lane] * before + taps_ref[1:2, lane] * lifted + taps_ref[2:3, lane] * after
            hidden = jax.nn.gelu(conv) * (product[rows, wide:] * gs_ref[:, lane])
            hidden_ref[rows, lane] = hidden.astype(hidden_ref.dtype)
        return carry

    lax.fori_loop(0, hidden_ref.shape[1] // wide, tile, 0)


def hidden_of(spot, x, up_scale, gate_scale, conv_weight, parts):
    rows, width = x.shape
    total = parts[0].shape[2]
    return pl.pallas_call(
        hidden_kernel,
        out_shape=jax.ShapeDtypeStruct((rows, total), jnp.bfloat16),
        in_specs=[in_smem(), *in_vmem(4 + len(parts))],
        out_specs=in_vmem()[0],
        scratch_shapes=[pltpu.VMEM((width, 256), jnp.bfloat16)],
        compiler_params=params(),
        cost_estimate=cost(4 * rows * width * total, 4 * rows * width),
        name="hidden",
    )(spot, x, up_scale[None], gate_scale[None], conv_weight, *near(*parts))


def down_kernel(spot_ref, hidden_ref, *refs):
    parts, (theirs_ref, mine_ref, weight_ref) = refs[:-3], refs[-3:]
    size = parts[0].shape[1]
    near = spot_ref[0] ^ (spot_ref[1] * 16)
    for p, part, j, flip in blocks_of(parts, orders_of("d")):
        owner = near ^ flip
        block = (owner & 15) * 2 + p

        @pl.when(owner >= 16)
        def _(part=part, j=j, block=block):
            weight_ref[at(block, size), :] = part[j]

        @pl.when(owner < 16)
        def _(part=part, j=j, block=block):
            mine_ref[at(block, size), :] = part[j]

    theirs_ref[...] = nt_dot(hidden_ref[...], weight_ref[...]).astype(theirs_ref.dtype)


def down_theirs(spot, hidden, parts, width):
    rows, depth = hidden.shape
    half = width // 2
    like = lambda *shape: jax.ShapeDtypeStruct(shape, jnp.bfloat16)
    return pl.pallas_call(
        down_kernel,
        out_shape=(like(rows, half), like(half, depth)),
        in_specs=[in_smem(), *in_vmem(1 + len(parts))],
        out_specs=in_vmem(2),
        scratch_shapes=[pltpu.VMEM((half, depth), jnp.bfloat16)],
        compiler_params=params(),
        cost_estimate=cost(rows * depth * width, 4 * rows * depth),
        name="down_theirs",
    )(spot, hidden, *near(*parts))


def terms_kernel(left_ref, right_ref, terms_ref):
    terms_ref[...] = nt_dot(left_ref[...], right_ref[...]).astype(terms_ref.dtype)


def terms_of(left, right):
    rows, depth = left.shape
    half = right.shape[0]
    return pl.pallas_call(
        terms_kernel,
        out_shape=jax.ShapeDtypeStruct((rows, half), jnp.bfloat16),
        in_specs=in_vmem(2),
        out_specs=in_vmem()[0],
        compiler_params=params(),
        cost_estimate=cost(2 * rows * depth * half, 4 * rows * half),
        name="down_mine",
    )(left, right)


def final_kernel(middle_ref, mine_ref, theirs_ref, scale_ref, out_ref):
    rows = at(pl.program_id(0), out_ref.shape[0])
    total = mine_ref[rows].astype(jnp.float32) + theirs_ref[rows].astype(jnp.float32)
    out_ref[...] = (middle_ref[rows].astype(jnp.float32) + total * scale_ref[...]).astype(out_ref.dtype)


def final_of(middle, mine, theirs, scale):
    rows, half = middle.shape
    return pl.pallas_call(
        final_kernel,
        grid=(4,),
        out_shape=jax.ShapeDtypeStruct((rows, half), jnp.bfloat16),
        in_specs=in_vmem(4),
        out_specs=pl.BlockSpec((rows // 4, half), lambda i: (i, 0)),
        compiler_params=params(8),
        cost_estimate=cost(0, 8 * rows * half),
        name="final",
    )(middle, mine, theirs, scale[None])


def per_device(
    layer_in,
    mix_gain,
    pool_weight,
    pool_scale,
    out_weight,
    out_scale,
    channel_gain,
    up_weight,
    up_scale,
    gate_weight,
    gate_scale,
    conv_weight,
    down_weight,
    down_scale,
):
    _, half = layer_in.shape
    me = lax.axis_index("tp")
    width = half * lax.axis_size("tp")
    cols = out_weight.shape[1]
    spot = jnp.stack([lax.axis_index(FS), me]).astype(jnp.int32)
    out_t = out_weight.astype(jnp.bfloat16).T
    pool_t = pool_weight.astype(jnp.bfloat16).transpose(2, 0, 1).reshape(-1, half)
    mixer_part = jnp.concatenate([out_t, pool_t], axis=0)
    lanes = half // 2
    mixer = gathered_over_fs(mixer_part[:, :lanes], "ma", 2) + gathered_over_fs(mixer_part[:, lanes:], "mb", 2)
    wide = gathered_over_fs(up_weight.astype(jnp.bfloat16), "u", 1)
    wide += gathered_over_fs(gate_weight.astype(jnp.bfloat16), "g", 1)
    down = gathered_over_fs(down_weight.astype(jnp.bfloat16).T, "d", 1)

    squares = squares_of(layer_in)
    own_gain = channel_gain[None]
    other_gain = from_partner(own_gain)
    pooled = pooled_of(spot, layer_in, squares, from_partner(squares), mix_gain)
    theirs, grouped, out_whole = mixer_theirs(spot, pooled, pool_scale, mixer, cols, width)
    theirs = from_partner(theirs)
    mine = mine_of(spot, grouped, out_whole)
    middle = middle_of(layer_in, mine, theirs, out_scale)
    chan_normed = normed_of(spot, middle, from_partner(middle), own_gain, other_gain)
    hidden = hidden_of(spot, chan_normed, up_scale, gate_scale, conv_weight, wide)
    theirs, down_mine = down_theirs(spot, hidden, down, width)
    theirs = from_partner(theirs)
    return final_of(middle, terms_of(hidden, down_mine), theirs, down_scale)


def solution(mesh):
    torus = Mesh(
        mesh.devices.reshape(mesh.shape["rep"], 2, 4, 4, mesh.shape["tp"]),
        ("rep", "fs_0", "fs_1", "fs_2", "tp"),
    )
    in_specs = (
        P(REP_FS, "tp"),
        P("tp"),
        P("tp", None, FS),
        P("tp", None),
        P("tp", FS),
        P("tp"),
        P("tp"),
        P(FS, "tp"),
        P("tp"),
        P(FS, "tp"),
        P("tp"),
        P(None, "tp"),
        P("tp", FS),
        P("tp"),
    )
    out_specs = P(REP_FS, "tp")
    return jax.shard_map(per_device, mesh=torus, in_specs=in_specs, out_specs=out_specs, check_vma=False)
```

```python
import functools
import math

import jax
import jax.numpy as jnp
from jax import lax
from jax.experimental import pallas as pl
from jax.experimental.pallas import tpu as pltpu
from jax.sharding import Mesh
from jax.sharding import PartitionSpec as P


LENGTH = 256
FS = ("fs_0", "fs_1", "fs_2")
REP_FS = ("rep", "fs_0", "fs_1", "fs_2")
EPS = 1e-06
GELU = (2 / math.pi) ** 0.5
SWAP = ((0, 1), (1, 0))


def from_partner(array):
    return lax.ppermute(array, "tp", SWAP)


def nt_dot(left, right):
    return lax.dot_general(left, right, (((1,), (1,)), ((), ())), preferred_element_type=jnp.float32)


LINKS = {
    "xa": ("fs_2", 1, 1),
    "xb": ("fs_2", 3, 3),
    "ya": ("fs_1", 1, 4),
    "yb": ("fs_1", 3, 12),
    "za": (("rep", "fs_0"), 1, 16),
    "zb": (("rep", "fs_0"), 3, 16),
}
PLANS = {
    "ma": ("yb zb ya", ("xa xb", "xb xa",)),
    "mb": ("ya xb xa", ("yb za", "za yb",)),
    "u": ("xb xa yb", ("zb ya", "ya za",)),
    "g": ("ya xb za", ("xa yb", "yb xa",)),
    "d": ("yb xa ya", ("zb xb", "xb zb",)),
}
UP_PARTS = ("u",)
GATE_PARTS = ("g",)
CHUNK = 4


def orders_of(*names):
    return tuple(f"{PLANS[name][0]} {end}" for name in names for end in PLANS[name][1])


def across(array, link):
    axes, flip, _ = LINKS[link]
    return lax.ppermute(array, axes, [(k, k ^ flip) for k in range(4)])


def stack_kernel(dim, first_ref, second_ref, *both_refs):
    count = first_ref.shape[0]
    size = both_refs[0].shape[dim]
    for k, both_ref in enumerate(both_refs):
        cut = slice(k * size, (k + 1) * size)
        place = (slice(None), cut) if dim == 1 else (slice(None), slice(None), cut)
        both_ref[:count] = first_ref[place]
        both_ref[count:] = second_ref[place]


def stacked(first, second, dim=1, pieces=1):
    count, *block = first.shape
    block[dim - 1] //= pieces
    return pl.pallas_call(
        functools.partial(stack_kernel, dim),
        out_shape=[pltpu.VMEM((2 * count, *block), first.dtype)] * pieces,
        in_specs=in_vmem(2),
        out_specs=in_vmem(pieces),
        compiler_params=params(4),
        cost_estimate=cost(0, 4 * first.size * 2),
        name="stack",
    )(*near(first, second))


def gathered_over_fs(group, name, dim):
    links, ends = PLANS[name]
    links = links.split()
    held = group[None]
    for step, link in enumerate(links):
        got = across(held, link)
        if step < len(links) - 1:
            (held,) = stacked(held, got)
    pairs = []
    for part, end in zip(stacked(held, got, dim, len(ends)), ends):
        near, far = end.split()
        got = across(part, near)
        (part,) = stacked(part, got)
        pairs += [part, across(part, far)]
    return pairs


def blocks_of(pairs, orders):
    for p, order in enumerate(orders):
        for j, flip in enumerate(flips(order)):
            side, place = divmod(j, pairs[2 * p].shape[0])
            yield p, pairs[2 * p + side], place, flip


def flips(order):
    found = [0]
    for link in order.split():
        found = found + [k ^ LINKS[link][2] for k in found]
    return found


def at(start, size):
    return pl.ds(pl.multiple_of(start * size, size), size)


def in_vmem(count=1):
    return [pl.BlockSpec(memory_space=pltpu.VMEM)] * count


def near(*arrays):
    return [pltpu.with_memory_space_constraint(array, pltpu.VMEM) for array in arrays]


def in_smem():
    return pl.BlockSpec(memory_space=pltpu.SMEM)


def params(mib=16):
    return pltpu.CompilerParams(vmem_limit_bytes=mib << 20)


def cost(flops, moved):
    return pl.CostEstimate(flops=flops, bytes_accessed=moved, transcendentals=0)


def squares_kernel(x_ref, squares_ref):
    for n in range(x_ref.shape[0] // LENGTH):
        seq = slice(n * LENGTH, (n + 1) * LENGTH)
        x = x_ref[seq].astype(jnp.float32)
        squares_ref[seq] = jnp.broadcast_to(jnp.sum(x * x, axis=1, keepdims=True), (LENGTH, 128))


def squares_of(x):
    return pl.pallas_call(
        squares_kernel,
        out_shape=jax.ShapeDtypeStruct((x.shape[0], 128), jnp.float32),
        in_specs=in_vmem(),
        out_specs=in_vmem()[0],
        compiler_params=params(8),
        cost_estimate=cost(0, 2 * x.size),
        name="squares",
    )(x)


def pool_kernel(spot_ref, x_ref, own_ref, other_ref, gain_ref, pooled_ref):
    rows, half = x_ref.shape
    groups = 2
    span = half // groups
    place = lax.broadcasted_iota(jnp.int32, (LENGTH, LENGTH), 0)
    other = lax.broadcasted_iota(jnp.int32, (LENGTH, LENGTH), 1)
    for k in range(groups):
        reach = jnp.left_shift(jnp.int32(1), spot_ref[1] * groups + k)
        lower = jnp.maximum(place - reach, 0)
        upper = jnp.minimum(place + reach, LENGTH)
        band = jnp.where((other >= lower) & (other < upper), 1.0, 0.0).astype(jnp.bfloat16)
        count = (upper - lower)[:, :1].astype(jnp.float32)
        lane = slice(k * span, (k + 1) * span)
        for n in range(rows // LENGTH):
            seq = slice(n * LENGTH, (n + 1) * LENGTH)
            squares = own_ref[seq, :1] + other_ref[seq, :1]
            scale = lax.rsqrt(squares / (2 * half) + EPS)
            normed = x_ref[seq, lane].astype(jnp.float32) * scale * gain_ref[:, lane].astype(jnp.float32)
            normed = normed.astype(jnp.bfloat16)
            total = jnp.dot(band, normed, preferred_element_type=jnp.float32)
            pooled_ref[seq, lane] = (total / count - normed.astype(jnp.float32)).astype(jnp.bfloat16)


def pooled_of(spot, x, own, other, gain):
    return pl.pallas_call(
        pool_kernel,
        out_shape=jax.ShapeDtypeStruct(x.shape, jnp.bfloat16),
        in_specs=[in_smem(), *in_vmem(4)],
        out_specs=in_vmem()[0],
        compiler_params=params(8),
        cost_estimate=cost(2 * LENGTH * x.size, 4 * x.size),
        name="pool",
    )(spot, x, own, other, gain[None])


def middle_kernel(x_ref, mine_ref, theirs_ref, scale_ref, middle_ref):
    total = mine_ref[...].astype(jnp.float32) + theirs_ref[...].astype(jnp.float32)
    middle_ref[...] = (x_ref[...].astype(jnp.float32) + total * scale_ref[...]).astype(jnp.bfloat16)


def middle_of(x, mine, theirs, scale):
    return pl.pallas_call(
        middle_kernel,
        out_shape=jax.ShapeDtypeStruct(x.shape, jnp.bfloat16),
        in_specs=in_vmem(4),
        out_specs=in_vmem()[0],
        compiler_params=params(8),
        cost_estimate=cost(0, 8 * x.size),
        name="middle",
    )(x, mine, theirs, scale[None])


def norm_kernel(spot_ref, own_ref, other_ref, own_gain_ref, other_gain_ref, normed_ref):
    rows, half = own_ref.shape
    for n in range(rows // LENGTH):
        seq = slice(n * LENGTH, (n + 1) * LENGTH)
        sides = [ref[seq].astype(jnp.float32) for ref in (own_ref, other_ref)]
        squares = sum(jnp.sum(side * side, axis=1, keepdims=True) for side in sides)
        scale = lax.rsqrt(squares / (2 * half) + EPS)
        for core, side, gain in zip((spot_ref[1], 1 - spot_ref[1]), sides, (own_gain_ref, other_gain_ref)):
            normed_ref[seq, at(core, half)] = (side * scale * gain[...].astype(jnp.float32)).astype(jnp.bfloat16)


def normed_of(spot, own, other, own_gain, other_gain):
    rows, half = own.shape
    return pl.pallas_call(
        norm_kernel,
        out_shape=jax.ShapeDtypeStruct((rows, 2 * half), jnp.bfloat16),
        in_specs=[in_smem(), *in_vmem(4)],
        out_specs=in_vmem()[0],
        compiler_params=params(8),
        cost_estimate=cost(0, 8 * own.size),
        name="norm",
    )(spot, own, other, own_gain, other_gain)


def theirs_kernel(cols, spot_ref, pooled_ref, scale_ref, *refs):
    parts, (theirs_ref, grouped_ref, out_ref, pool_ref) = refs[:-4], refs[-4:]
    groups, group_width = pool_ref.shape[:2]
    half = groups * group_width
    lanes = parts[0].shape[2]
    extra = parts[0].shape[1] - cols
    for p, part, j, flip in blocks_of(parts, orders_of("ma", "mb")):
        group, place = divmod(p * lanes, group_width)
        owner = spot_ref[0] ^ flip
        out_ref[at(owner, cols), p * lanes : (p + 1) * lanes] = part[j, :cols]
        pool_ref[group, at(owner, extra), place : place + lanes] = part[j, cols:]
    for k in range(groups):
        span = slice(k * group_width, (k + 1) * group_width)
        product = nt_dot(pooled_ref[:, span], pool_ref[k])
        grouped_ref[:, span] = (product * scale_ref[k : k + 1]).astype(jnp.bfloat16)
    theirs_ref[...] = nt_dot(grouped_ref[...], out_ref[at(1 - spot_ref[1], half), :]).astype(jnp.bfloat16)


def mixer_theirs(spot, pooled, pool_scale, parts, cols, width):
    rows, half = pooled.shape
    groups, group_width = pool_scale.shape
    like = lambda *shape: jax.ShapeDtypeStruct(shape, jnp.bfloat16)
    return pl.pallas_call(
        functools.partial(theirs_kernel, cols),
        out_shape=(like(rows, half), like(rows, half), like(width, half)),
        in_specs=[in_smem(), *in_vmem(2 + len(parts))],
        out_specs=in_vmem(3),
        scratch_shapes=[pltpu.VMEM((groups, group_width, group_width), jnp.bfloat16)],
        compiler_params=params(),
        cost_estimate=cost(2 * rows * half * (half + group_width), 4 * rows * half),
        name="mixer_theirs",
    )(spot, pooled, pool_scale, *near(*parts))


def mine_kernel(spot_ref, left_ref, right_ref, mine_ref):
    half = mine_ref.shape[1]
    mine_ref[...] = nt_dot(left_ref[...], right_ref[at(spot_ref[1], half), :]).astype(jnp.bfloat16)


def mine_of(spot, left, right):
    rows, depth = left.shape
    half = right.shape[0] // 2
    return pl.pallas_call(
        mine_kernel,
        out_shape=jax.ShapeDtypeStruct((rows, half), jnp.bfloat16),
        in_specs=[in_smem(), *in_vmem(2)],
        out_specs=in_vmem()[0],
        compiler_params=params(),
        cost_estimate=cost(2 * rows * depth * half, 4 * rows * half),
    )(spot, left, right)


def weight_tile(spot_ref, parts, names, weight_ref, lane, wide):
    size = parts[0].shape[1]
    for p, part, j, flip in blocks_of(parts, orders_of(*names)):
        weight_ref[at((spot_ref[0] ^ flip) * 2 + p, size), :wide] = part[j, :, lane]


def over_tiles(total, step, tile):
    def whole(i, carry):
        tile(at(i, step), step)
        return carry

    lax.fori_loop(0, total // step, whole, 0)
    if total % step:
        tile(slice(total // step * step, total), total % step)


def up_kernel(spot_ref, x_ref, us_ref, taps_ref, *refs):
    parts, (act_ref, weight_ref) = refs[:-2], refs[-2:]
    span = CHUNK * LENGTH

    def tile(lane, wide):
        weight_tile(spot_ref, parts, UP_PARTS, weight_ref, lane, wide)
        row = lax.broadcasted_iota(jnp.int32, (LENGTH, wide), 0)
        early, same, late = (taps_ref[n : n + 1, lane] * us_ref[:, lane] for n in range(3))
        for start in range(0, x_ref.shape[0], span):
            product = jnp.dot(x_ref[start : start + span], weight_ref[:, :wide], preferred_element_type=jnp.float32)
            for k in range(CHUNK):
                lifted = product[k * LENGTH : (k + 1) * LENGTH]
                before = jnp.where(row == 0, 0.0, pltpu.roll(lifted, 1, 0))
                after = jnp.where(row == LENGTH - 1, 0.0, pltpu.roll(lifted, LENGTH - 1, 0))
                conv = early * before + same * lifted + late * after
                slope = conv * (GELU + (GELU * 0.044715) * (conv * conv))
                half = 0.5 * conv
                rows = slice(start + k * LENGTH, start + (k + 1) * LENGTH)
                act_ref[rows, lane] = (half + half * jnp.tanh(slope)).astype(act_ref.dtype)

    over_tiles(act_ref.shape[1], weight_ref.shape[1], tile)


def gate_kernel(spot_ref, x_ref, gs_ref, act_ref, *refs):
    parts, (hidden_ref, weight_ref) = refs[:-2], refs[-2:]
    span = CHUNK * LENGTH

    def tile(lane, wide):
        weight_tile(spot_ref, parts, GATE_PARTS, weight_ref, lane, wide)
        for start in range(0, x_ref.shape[0], span):
            rows = slice(start, start + span)
            gated = jnp.dot(x_ref[rows], weight_ref[:, :wide], preferred_element_type=jnp.float32) * gs_ref[:, lane]
            hidden_ref[rows, lane] = (act_ref[rows, lane].astype(jnp.float32) * gated).astype(hidden_ref.dtype)

    over_tiles(hidden_ref.shape[1], weight_ref.shape[1], tile)


def wide_of(kernel, spot, x, others, parts):
    rows, width = x.shape
    total = parts[0].shape[2]
    return pl.pallas_call(
        kernel,
        out_shape=jax.ShapeDtypeStruct((rows, total), jnp.bfloat16),
        in_specs=[in_smem(), *in_vmem(1 + len(others) + len(parts))],
        out_specs=in_vmem()[0],
        scratch_shapes=[pltpu.VMEM((width, 256), jnp.bfloat16)],
        compiler_params=params(),
        cost_estimate=cost(2 * rows * width * total, 4 * rows * width),
    )(spot, x, *others, *near(*parts))


def down_kernel(spot_ref, hidden_ref, *refs):
    parts, (theirs_ref, mine_ref, weight_ref) = refs[:-3], refs[-3:]
    size = parts[0].shape[1]
    near = spot_ref[0] ^ (spot_ref[1] * 16)
    for p, part, j, flip in blocks_of(parts, orders_of("d")):
        owner = near ^ flip
        block = (owner & 15) * 2 + p

        @pl.when(owner >= 16)
        def _(part=part, j=j, block=block):
            weight_ref[at(block, size), :] = part[j]

        @pl.when(owner < 16)
        def _(part=part, j=j, block=block):
            mine_ref[at(block, size), :] = part[j]

    theirs_ref[...] = nt_dot(hidden_ref[...], weight_ref[...]).astype(theirs_ref.dtype)


def down_theirs(spot, hidden, parts, width):
    rows, depth = hidden.shape
    half = width // 2
    like = lambda *shape: jax.ShapeDtypeStruct(shape, jnp.bfloat16)
    return pl.pallas_call(
        down_kernel,
        out_shape=(like(rows, half), like(half, depth)),
        in_specs=[in_smem(), *in_vmem(1 + len(parts))],
        out_specs=in_vmem(2),
        scratch_shapes=[pltpu.VMEM((half, depth), jnp.bfloat16)],
        compiler_params=params(),
        cost_estimate=cost(rows * depth * width, 4 * rows * depth),
        name="down_theirs",
    )(spot, hidden, *near(*parts))


def terms_kernel(left_ref, right_ref, terms_ref):
    terms_ref[...] = nt_dot(left_ref[...], right_ref[...]).astype(terms_ref.dtype)


def terms_of(left, right):
    rows, depth = left.shape
    half = right.shape[0]
    return pl.pallas_call(
        terms_kernel,
        out_shape=jax.ShapeDtypeStruct((rows, half), jnp.bfloat16),
        in_specs=in_vmem(2),
        out_specs=in_vmem()[0],
        compiler_params=params(),
        cost_estimate=cost(2 * rows * depth * half, 4 * rows * half),
        name="down_mine",
    )(left, right)


def final_kernel(middle_ref, mine_ref, theirs_ref, scale_ref, out_ref):
    rows = at(pl.program_id(0), out_ref.shape[0])
    total = mine_ref[rows].astype(jnp.float32) + theirs_ref[rows].astype(jnp.float32)
    out_ref[...] = (middle_ref[rows].astype(jnp.float32) + total * scale_ref[...]).astype(out_ref.dtype)


def final_of(middle, mine, theirs, scale):
    rows, half = middle.shape
    return pl.pallas_call(
        final_kernel,
        grid=(4,),
        out_shape=jax.ShapeDtypeStruct((rows, half), jnp.bfloat16),
        in_specs=in_vmem(4),
        out_specs=pl.BlockSpec((rows // 4, half), lambda i: (i, 0)),
        compiler_params=params(8),
        cost_estimate=cost(0, 8 * rows * half),
        name="final",
    )(middle, mine, theirs, scale[None])


def per_device(
    layer_in,
    mix_gain,
    pool_weight,
    pool_scale,
    out_weight,
    out_scale,
    channel_gain,
    up_weight,
    up_scale,
    gate_weight,
    gate_scale,
    conv_weight,
    down_weight,
    down_scale,
):
    _, half = layer_in.shape
    me = lax.axis_index("tp")
    width = half * lax.axis_size("tp")
    cols = out_weight.shape[1]
    spot = jnp.stack([lax.axis_index(FS), me]).astype(jnp.int32)
    out_t = out_weight.astype(jnp.bfloat16).T
    pool_t = pool_weight.astype(jnp.bfloat16).transpose(2, 0, 1).reshape(-1, half)
    mixer_part = jnp.concatenate([out_t, pool_t], axis=0)
    lanes = half // 2
    mixer = gathered_over_fs(mixer_part[:, :lanes], "ma", 2) + gathered_over_fs(mixer_part[:, lanes:], "mb", 2)
    up = gathered_over_fs(up_weight.astype(jnp.bfloat16), "u", 1)
    gate = gathered_over_fs(gate_weight.astype(jnp.bfloat16), "g", 1)
    down = gathered_over_fs(down_weight.astype(jnp.bfloat16).T, "d", 1)

    squares = squares_of(layer_in)
    own_gain = channel_gain[None]
    other_gain = from_partner(own_gain)
    pooled = pooled_of(spot, layer_in, squares, from_partner(squares), mix_gain)
    theirs, grouped, out_whole = mixer_theirs(spot, pooled, pool_scale, mixer, cols, width)
    theirs = from_partner(theirs)
    mine = mine_of(spot, grouped, out_whole)
    middle = middle_of(layer_in, mine, theirs, out_scale)
    chan_normed = normed_of(spot, middle, from_partner(middle), own_gain, other_gain)
    act = wide_of(up_kernel, spot, chan_normed, (up_scale[None], conv_weight), up)
    hidden = wide_of(gate_kernel, spot, chan_normed, (gate_scale[None], act), gate)
    theirs, down_mine = down_theirs(spot, hidden, down, width)
    theirs = from_partner(theirs)
    return final_of(middle, terms_of(hidden, down_mine), theirs, down_scale)


def solution(mesh):
    torus = Mesh(
        mesh.devices.reshape(mesh.shape["rep"], 2, 4, 4, mesh.shape["tp"]),
        ("rep", "fs_0", "fs_1", "fs_2", "tp"),
    )
    in_specs = (
        P(REP_FS, "tp"),
        P("tp"),
        P("tp", None, FS),
        P("tp", None),
        P("tp", FS),
        P("tp"),
        P("tp"),
        P(FS, "tp"),
        P("tp"),
        P(FS, "tp"),
        P("tp"),
        P(None, "tp"),
        P("tp", FS),
        P("tp"),
    )
    out_specs = P(REP_FS, "tp")
    return jax.shard_map(per_device, mesh=torus, in_specs=in_specs, out_specs=out_specs, check_vma=False)
```

```python
import functools
import math

import jax
import jax.numpy as jnp
from jax import lax
from jax.experimental import pallas as pl
from jax.experimental.pallas import tpu as pltpu
from jax.sharding import Mesh
from jax.sharding import PartitionSpec as P


LENGTH = 256
FS = ("fs_0", "fs_1", "fs_2")
REP_FS = ("rep", "fs_0", "fs_1", "fs_2")
EPS = 1e-06
GELU = (2 / math.pi) ** 0.5
SWAP = ((0, 1), (1, 0))


def from_partner(array):
    return lax.ppermute(array, "tp", SWAP)


def nt_dot(left, right):
    return lax.dot_general(left, right, (((1,), (1,)), ((), ())), preferred_element_type=jnp.float32)


LINKS = {
    "xa": ("fs_2", 1, 1),
    "xb": ("fs_2", 3, 3),
    "ya": ("fs_1", 1, 4),
    "yb": ("fs_1", 3, 12),
    "za": (("rep", "fs_0"), 1, 16),
    "zb": (("rep", "fs_0"), 3, 16),
}
PLANS = {
    "ma": ("yb zb ya", ("xa xb", "xb xa",)),
    "mb": ("ya xb xa", ("yb za", "za yb",)),
    "u": ("xb xa yb", ("zb ya", "ya za",)),
    "g": ("ya xb za", ("xa yb", "yb xa",)),
    "d": ("yb xa ya", ("zb xb", "xb zb",)),
}
UP_PARTS = ("u",)
GATE_PARTS = ("g",)
CHUNK = 4


def orders_of(*names):
    return tuple(f"{PLANS[name][0]} {end}" for name in names for end in PLANS[name][1])


def across(array, link):
    axes, flip, _ = LINKS[link]
    return lax.ppermute(array, axes, [(k, k ^ flip) for k in range(4)])


def stack_kernel(dim, first_ref, second_ref, *both_refs):
    count = first_ref.shape[0]
    size = both_refs[0].shape[dim]
    for k, both_ref in enumerate(both_refs):
        cut = slice(k * size, (k + 1) * size)
        place = (slice(None), cut) if dim == 1 else (slice(None), slice(None), cut)
        both_ref[:count] = first_ref[place]
        both_ref[count:] = second_ref[place]


def stacked(first, second, dim=1, pieces=1):
    count, *block = first.shape
    block[dim - 1] //= pieces
    return pl.pallas_call(
        functools.partial(stack_kernel, dim),
        out_shape=[pltpu.VMEM((2 * count, *block), first.dtype)] * pieces,
        in_specs=in_vmem(2),
        out_specs=in_vmem(pieces),
        compiler_params=params(4),
        cost_estimate=cost(0, 4 * first.size * 2),
        name="stack",
    )(*near(first, second))


def gathered_over_fs(group, name, dim):
    links, ends = PLANS[name]
    links = links.split()
    held = group[None]
    for step, link in enumerate(links):
        got = across(held, link)
        if step < len(links) - 1:
            (held,) = stacked(held, got)
    pairs = []
    for part, end in zip(stacked(held, got, dim, len(ends)), ends):
        near, far = end.split()
        got = across(part, near)
        (part,) = stacked(part, got)
        pairs += [part, across(part, far)]
    return pairs


def blocks_of(pairs, orders):
    for p, order in enumerate(orders):
        for j, flip in enumerate(flips(order)):
            side, place = divmod(j, pairs[2 * p].shape[0])
            yield p, pairs[2 * p + side], place, flip


def flips(order):
    found = [0]
    for link in order.split():
        found = found + [k ^ LINKS[link][2] for k in found]
    return found


def at(start, size):
    return pl.ds(pl.multiple_of(start * size, size), size)


def in_vmem(count=1):
    return [pl.BlockSpec(memory_space=pltpu.VMEM)] * count


def near(*arrays):
    return [pltpu.with_memory_space_constraint(array, pltpu.VMEM) for array in arrays]


def in_smem():
    return pl.BlockSpec(memory_space=pltpu.SMEM)


def params(mib=16):
    return pltpu.CompilerParams(vmem_limit_bytes=mib << 20)


def cost(flops, moved):
    return pl.CostEstimate(flops=flops, bytes_accessed=moved, transcendentals=0)


def squares_kernel(x_ref, squares_ref):
    for n in range(x_ref.shape[0] // LENGTH):
        seq = slice(n * LENGTH, (n + 1) * LENGTH)
        x = x_ref[seq].astype(jnp.float32)
        squares_ref[seq] = jnp.broadcast_to(jnp.sum(x * x, axis=1, keepdims=True), (LENGTH, 128))


def squares_of(x):
    return pl.pallas_call(
        squares_kernel,
        out_shape=jax.ShapeDtypeStruct((x.shape[0], 128), jnp.float32),
        in_specs=in_vmem(),
        out_specs=in_vmem()[0],
        compiler_params=params(8),
        cost_estimate=cost(0, 2 * x.size),
        name="squares",
    )(x)


def pool_kernel(spot_ref, x_ref, own_ref, other_ref, gain_ref, pooled_ref):
    rows, half = x_ref.shape
    groups = 2
    span = half // groups
    place = lax.broadcasted_iota(jnp.int32, (LENGTH, LENGTH), 0)
    other = lax.broadcasted_iota(jnp.int32, (LENGTH, LENGTH), 1)
    for k in range(groups):
        reach = jnp.left_shift(jnp.int32(1), spot_ref[1] * groups + k)
        lower = jnp.maximum(place - reach, 0)
        upper = jnp.minimum(place + reach, LENGTH)
        band = jnp.where((other >= lower) & (other < upper), 1.0, 0.0).astype(jnp.bfloat16)
        count = (upper - lower)[:, :1].astype(jnp.float32)
        lane = slice(k * span, (k + 1) * span)
        for n in range(rows // LENGTH):
            seq = slice(n * LENGTH, (n + 1) * LENGTH)
            squares = own_ref[seq, :1] + other_ref[seq, :1]
            scale = lax.rsqrt(squares / (2 * half) + EPS)
            normed = x_ref[seq, lane].astype(jnp.float32) * scale * gain_ref[:, lane].astype(jnp.float32)
            normed = normed.astype(jnp.bfloat16)
            total = jnp.dot(band, normed, preferred_element_type=jnp.float32)
            pooled_ref[seq, lane] = (total / count - normed.astype(jnp.float32)).astype(jnp.bfloat16)


def pooled_of(spot, x, own, other, gain):
    return pl.pallas_call(
        pool_kernel,
        out_shape=jax.ShapeDtypeStruct(x.shape, jnp.bfloat16),
        in_specs=[in_smem(), *in_vmem(4)],
        out_specs=in_vmem()[0],
        compiler_params=params(8),
        cost_estimate=cost(2 * LENGTH * x.size, 4 * x.size),
        name="pool",
    )(spot, x, own, other, gain[None])


def middle_kernel(x_ref, mine_ref, theirs_ref, scale_ref, middle_ref):
    total = mine_ref[...].astype(jnp.float32) + theirs_ref[...].astype(jnp.float32)
    middle_ref[...] = (x_ref[...].astype(jnp.float32) + total * scale_ref[...]).astype(jnp.bfloat16)


def middle_of(x, mine, theirs, scale):
    return pl.pallas_call(
        middle_kernel,
        out_shape=jax.ShapeDtypeStruct(x.shape, jnp.bfloat16),
        in_specs=in_vmem(4),
        out_specs=in_vmem()[0],
        compiler_params=params(8),
        cost_estimate=cost(0, 8 * x.size),
        name="middle",
    )(x, mine, theirs, scale[None])


def norm_kernel(spot_ref, own_ref, other_ref, own_gain_ref, other_gain_ref, normed_ref):
    rows, half = own_ref.shape
    for n in range(rows // LENGTH):
        seq = slice(n * LENGTH, (n + 1) * LENGTH)
        sides = [ref[seq].astype(jnp.float32) for ref in (own_ref, other_ref)]
        squares = sum(jnp.sum(side * side, axis=1, keepdims=True) for side in sides)
        scale = lax.rsqrt(squares / (2 * half) + EPS)
        for core, side, gain in zip((spot_ref[1], 1 - spot_ref[1]), sides, (own_gain_ref, other_gain_ref)):
            normed_ref[seq, at(core, half)] = (side * scale * gain[...].astype(jnp.float32)).astype(jnp.bfloat16)


def normed_of(spot, own, other, own_gain, other_gain):
    rows, half = own.shape
    return pl.pallas_call(
        norm_kernel,
        out_shape=jax.ShapeDtypeStruct((rows, 2 * half), jnp.bfloat16),
        in_specs=[in_smem(), *in_vmem(4)],
        out_specs=in_vmem()[0],
        compiler_params=params(8),
        cost_estimate=cost(0, 8 * own.size),
        name="norm",
    )(spot, own, other, own_gain, other_gain)


def theirs_kernel(cols, spot_ref, pooled_ref, scale_ref, *refs):
    parts, (theirs_ref, grouped_ref, out_ref, pool_ref) = refs[:-4], refs[-4:]
    groups, group_width = pool_ref.shape[:2]
    half = groups * group_width
    lanes = parts[0].shape[2]
    extra = parts[0].shape[1] - cols
    for p, part, j, flip in blocks_of(parts, orders_of("ma", "mb")):
        group, place = divmod(p * lanes, group_width)
        owner = spot_ref[0] ^ flip
        out_ref[at(owner, cols), p * lanes : (p + 1) * lanes] = part[j, :cols]
        pool_ref[group, at(owner, extra), place : place + lanes] = part[j, cols:]
    for k in range(groups):
        span = slice(k * group_width, (k + 1) * group_width)
        product = nt_dot(pooled_ref[:, span], pool_ref[k])
        grouped_ref[:, span] = (product * scale_ref[k : k + 1]).astype(jnp.bfloat16)
    theirs_ref[...] = nt_dot(grouped_ref[...], out_ref[at(1 - spot_ref[1], half), :]).astype(jnp.bfloat16)


def mixer_theirs(spot, pooled, pool_scale, parts, cols, width):
    rows, half = pooled.shape
    groups, group_width = pool_scale.shape
    like = lambda *shape: jax.ShapeDtypeStruct(shape, jnp.bfloat16)
    return pl.pallas_call(
        functools.partial(theirs_kernel, cols),
        out_shape=(like(rows, half), like(rows, half), like(width, half)),
        in_specs=[in_smem(), *in_vmem(2 + len(parts))],
        out_specs=in_vmem(3),
        scratch_shapes=[pltpu.VMEM((groups, group_width, group_width), jnp.bfloat16)],
        compiler_params=params(),
        cost_estimate=cost(2 * rows * half * (half + group_width), 4 * rows * half),
        name="mixer_theirs",
    )(spot, pooled, pool_scale, *near(*parts))


def mine_kernel(spot_ref, left_ref, right_ref, mine_ref):
    half = mine_ref.shape[1]
    mine_ref[...] = nt_dot(left_ref[...], right_ref[at(spot_ref[1], half), :]).astype(jnp.bfloat16)


def mine_of(spot, left, right):
    rows, depth = left.shape
    half = right.shape[0] // 2
    return pl.pallas_call(
        mine_kernel,
        out_shape=jax.ShapeDtypeStruct((rows, half), jnp.bfloat16),
        in_specs=[in_smem(), *in_vmem(2)],
        out_specs=in_vmem()[0],
        compiler_params=params(),
        cost_estimate=cost(2 * rows * depth * half, 4 * rows * half),
    )(spot, left, right)


def weight_tile(spot_ref, parts, names, weight_ref, lane, wide):
    size = parts[0].shape[1]
    for p, part, j, flip in blocks_of(parts, orders_of(*names)):
        weight_ref[at((spot_ref[0] ^ flip) * 2 + p, size), :wide] = part[j, :, lane]


def over_tiles(total, step, tile):
    def whole(i, carry):
        tile(at(i, step), step)
        return carry

    lax.fori_loop(0, total // step, whole, 0)
    if total % step:
        tile(slice(total // step * step, total), total % step)


def up_kernel(spot_ref, x_ref, us_ref, taps_ref, *refs):
    parts, (act_ref, weight_ref) = refs[:-2], refs[-2:]
    span = CHUNK * LENGTH

    def tile(lane, wide):
        weight_tile(spot_ref, parts, UP_PARTS, weight_ref, lane, wide)
        row = lax.broadcasted_iota(jnp.int32, (LENGTH, wide), 0)
        early, same, late = (taps_ref[n : n + 1, lane] * us_ref[:, lane] for n in range(3))
        for start in range(0, x_ref.shape[0], span):
            product = jnp.dot(x_ref[start : start + span], weight_ref[:, :wide], preferred_element_type=jnp.float32)
            for k in range(CHUNK):
                lifted = product[k * LENGTH : (k + 1) * LENGTH]
                before = jnp.where(row == 0, 0.0, pltpu.roll(lifted, 1, 0))
                after = jnp.where(row == LENGTH - 1, 0.0, pltpu.roll(lifted, LENGTH - 1, 0))
                conv = early * before + same * lifted + late * after
                slope = conv * (GELU + (GELU * 0.044715) * (conv * conv))
                half = 0.5 * conv
                rows = slice(start + k * LENGTH, start + (k + 1) * LENGTH)
                act_ref[rows, lane] = (half + half * jnp.tanh(slope)).astype(act_ref.dtype)

    over_tiles(act_ref.shape[1], weight_ref.shape[1], tile)


def gate_kernel(spot_ref, x_ref, gs_ref, act_ref, *refs):
    parts, (hidden_ref, weight_ref) = refs[:-2], refs[-2:]
    span = CHUNK * LENGTH

    def tile(lane, wide):
        weight_tile(spot_ref, parts, GATE_PARTS, weight_ref, lane, wide)
        for start in range(0, x_ref.shape[0], span):
            rows = slice(start, start + span)
            gated = jnp.dot(x_ref[rows], weight_ref[:, :wide], preferred_element_type=jnp.float32) * gs_ref[:, lane]
            hidden_ref[rows, lane] = (act_ref[rows, lane].astype(jnp.float32) * gated).astype(hidden_ref.dtype)

    over_tiles(hidden_ref.shape[1], weight_ref.shape[1], tile)


def wide_of(kernel, spot, x, others, parts):
    rows, width = x.shape
    total = parts[0].shape[2]
    return pl.pallas_call(
        kernel,
        out_shape=jax.ShapeDtypeStruct((rows, total), jnp.bfloat16),
        in_specs=[in_smem(), *in_vmem(1 + len(others) + len(parts))],
        out_specs=in_vmem()[0],
        scratch_shapes=[pltpu.VMEM((width, 256), jnp.bfloat16)],
        compiler_params=params(),
        cost_estimate=cost(2 * rows * width * total, 4 * rows * width),
    )(spot, x, *others, *near(*parts))


def down_terms_kernel(side, spot_ref, hidden_ref, *refs):
    parts, (terms_ref, weight_ref) = refs[:-2], refs[-2:]
    count, size = parts[0].shape[:2]
    near_by = spot_ref[0] ^ (spot_ref[1] * 16)
    pick = (near_by >> 4) ^ side
    for p, order in enumerate(orders_of("d")):
        found = flips(order)
        for j, flip in enumerate(found):
            if flip & 16:
                continue
            (here, first), (there, second) = divmod(j, count), divmod(found.index(flip ^ 16), count)
            if here == there:
                block = parts[2 * p + here][first + (second - first) * pick]
            else:
                block = lax.select(pick == 1, parts[2 * p + there][second], parts[2 * p + here][first])
            weight_ref[at(((near_by ^ flip) & 15) * 2 + p, size), :] = block
    terms_ref[...] = nt_dot(hidden_ref[...], weight_ref[...]).astype(terms_ref.dtype)


def down_terms(side, spot, hidden, parts, width):
    rows, depth = hidden.shape
    half = width // 2
    return pl.pallas_call(
        functools.partial(down_terms_kernel, side),
        out_shape=jax.ShapeDtypeStruct((rows, half), jnp.bfloat16),
        in_specs=[in_smem(), *in_vmem(1 + len(parts))],
        out_specs=in_vmem()[0],
        scratch_shapes=[pltpu.VMEM((half, depth), jnp.bfloat16)],
        compiler_params=params(),
        cost_estimate=cost(2 * rows * depth * half, 4 * rows * depth),
    )(spot, hidden, *near(*parts))


def final_kernel(middle_ref, mine_ref, theirs_ref, scale_ref, out_ref):
    rows = at(pl.program_id(0), out_ref.shape[0])
    total = mine_ref[rows].astype(jnp.float32) + theirs_ref[rows].astype(jnp.float32)
    out_ref[...] = (middle_ref[rows].astype(jnp.float32) + total * scale_ref[...]).astype(out_ref.dtype)


def final_of(middle, mine, theirs, scale):
    rows, half = middle.shape
    return pl.pallas_call(
        final_kernel,
        grid=(4,),
        out_shape=jax.ShapeDtypeStruct((rows, half), jnp.bfloat16),
        in_specs=in_vmem(4),
        out_specs=pl.BlockSpec((rows // 4, half), lambda i: (i, 0)),
        compiler_params=params(8),
        cost_estimate=cost(0, 8 * rows * half),
        name="final",
    )(middle, mine, theirs, scale[None])


def per_device(
    layer_in,
    mix_gain,
    pool_weight,
    pool_scale,
    out_weight,
    out_scale,
    channel_gain,
    up_weight,
    up_scale,
    gate_weight,
    gate_scale,
    conv_weight,
    down_weight,
    down_scale,
):
    _, half = layer_in.shape
    me = lax.axis_index("tp")
    width = half * lax.axis_size("tp")
    cols = out_weight.shape[1]
    spot = jnp.stack([lax.axis_index(FS), me]).astype(jnp.int32)
    out_t = out_weight.astype(jnp.bfloat16).T
    pool_t = pool_weight.astype(jnp.bfloat16).transpose(2, 0, 1).reshape(-1, half)
    mixer_part = jnp.concatenate([out_t, pool_t], axis=0)
    lanes = half // 2
    mixer = gathered_over_fs(mixer_part[:, :lanes], "ma", 2) + gathered_over_fs(mixer_part[:, lanes:], "mb", 2)
    up = gathered_over_fs(up_weight.astype(jnp.bfloat16), "u", 1)
    gate = gathered_over_fs(gate_weight.astype(jnp.bfloat16), "g", 1)
    down = gathered_over_fs(down_weight.astype(jnp.bfloat16).T, "d", 1)

    squares = squares_of(layer_in)
    own_gain = channel_gain[None]
    other_gain = from_partner(own_gain)
    pooled = pooled_of(spot, layer_in, squares, from_partner(squares), mix_gain)
    theirs, grouped, out_whole = mixer_theirs(spot, pooled, pool_scale, mixer, cols, width)
    theirs = from_partner(theirs)
    mine = mine_of(spot, grouped, out_whole)
    middle = middle_of(layer_in, mine, theirs, out_scale)
    chan_normed = normed_of(spot, middle, from_partner(middle), own_gain, other_gain)
    act = wide_of(up_kernel, spot, chan_normed, (up_scale[None], conv_weight), up)
    hidden = wide_of(gate_kernel, spot, chan_normed, (gate_scale[None], act), gate)
    theirs = from_partner(down_terms(1, spot, hidden, down, width))
    mine = down_terms(0, spot, hidden, down, width)
    return final_of(middle, mine, theirs, down_scale)


def solution(mesh):
    torus = Mesh(
        mesh.devices.reshape(mesh.shape["rep"], 2, 4, 4, mesh.shape["tp"]),
        ("rep", "fs_0", "fs_1", "fs_2", "tp"),
    )
    in_specs = (
        P(REP_FS, "tp"),
        P("tp"),
        P("tp", None, FS),
        P("tp", None),
        P("tp", FS),
        P("tp"),
        P("tp"),
        P(FS, "tp"),
        P("tp"),
        P(FS, "tp"),
        P("tp"),
        P(None, "tp"),
        P("tp", FS),
        P("tp"),
    )
    out_specs = P(REP_FS, "tp")
    return jax.shard_map(per_device, mesh=torus, in_specs=in_specs, out_specs=out_specs, check_vma=False)
```
